32 devices in a mesh: sp: 4 (over z), fs: 4 (over y, x), tp: 2 (over core).
Axes of the slice: x: 2, y: 2, z: 4, core: 2. Of those that a mesh axis runs over, the one named last changes fastest.
Arguments:
- tokens: bfloat16 [4, 512, 4096], P('fs', 'sp'), may hold values from -6 to 6
- norm_gain: float32 [4096], replicated, may hold values from 0.1 to 1.9
- pool_proj: bfloat16 [4096, 1024], P(('sp', 'fs'), 'tp'), may hold values from -0.09375 to 0.09375
- query_proj: bfloat16 [4096, 1024], P(('sp', 'fs'), 'tp'), may hold values from -0.09375 to 0.09375
- key_proj: bfloat16 [4096, 1024], P(('sp', 'fs'), 'tp'), may hold values from -0.09375 to 0.09375
- value_proj: bfloat16 [4096, 1024], P(('sp', 'fs'), 'tp'), may hold values from -0.09375 to 0.09375
- pool_map: bfloat16 [4, 256, 256], replicated, may hold values from -0.375 to 0.375
- pool_scale: float32 [1024], replicated, may hold values from 0.1 to 1.9
- decay_rate: float32 [4], P('tp'), may hold values from 2e-05 to 0.034
- start_state: float32 [4, 4, 256, 256], P('fs', 'tp', 'sp'), may hold values from -96 to 96
- pool_back: bfloat16 [1024, 4096], P('tp', ('sp', 'fs')), may hold values from -0.125 to 0.125
- retention_back: bfloat16 [1024, 4096], P('tp', ('sp', 'fs')), may hold values from -0.125 to 0.125
Outputs:
- mixed: bfloat16 [4, 512, 4096], P('fs', ('sp', 'tp'))
The draws below stay inside these ranges and needn't reach their ends.
All inputs are finite; a program needn't handle non-finite values.
Results may differ from the reference program's by a relative error of at most 0.014.
Values may be sent and summed in bfloat16 or wider, within the bound.
A program may use at most 128 MiB of HBM per device.

```python
import jax
import jax.numpy as jnp
from jax import lax

DMODEL = 4096
GROUPS = 4
GROUP_DIM = 256
RET_HEADS = 4
HEAD_DIM = 256
BLOCK = 128
HALO = 16
POOL_WIDTH = 1024
RET_WIDTH = 1024
SEQS = 4
SEQ_LEN = 512


def draw_decay_rate(key, part):
    order_key, level_key = jax.random.split(jax.random.fold_in(key, 7))
    order = jax.random.permutation(order_key, RET_HEADS)
    quick = order < RET_HEADS // 2
    level = jax.random.uniform(level_key, (RET_HEADS,), jnp.float32)
    quick_rate = jnp.exp(jnp.log(0.01) + level * (jnp.log(1.0 / 30.0) - jnp.log(0.01)))
    slow_rate = jnp.exp(jnp.log(2e-05) + level * (jnp.log(0.00012) - jnp.log(2e-05)))
    return jnp.where(quick, quick_rate, slow_rate).astype(jnp.float32)


def levels(rng, dims, cuts, smallest, high):
    factor_of = 1.0
    for dim, parts in cuts:
        steps = jax.random.uniform(jax.random.fold_in(jax.random.fold_in(rng, 6), dim), (parts,), jnp.float32, smallest / len(cuts), high / len(cuts))
        factor_of = factor_of * jnp.repeat(jnp.exp(steps), dims[dim] // parts).reshape((-1,) + (1,) * (len(dims) - 1 - dim))
    return factor_of


def normal_values(stream_key, dims, spread, most, cuts=(), held_as=jnp.bfloat16):
    drawn = jax.random.normal(stream_key, dims, jnp.float32) * spread
    if len(cuts) > 0:
        drawn = levels(stream_key, dims, cuts, -0.22, 0.18) * drawn
    return jnp.clip(drawn, min=-most, max=most).astype(held_as)


def setup_inputs(seed: int = 0) -> dict:
    streams_of = jax.random.split(jax.random.key(seed), 13)
    tokens = normal_values(streams_of[0], (SEQS, SEQ_LEN, DMODEL), 1.0, 6.0, ((0, 4), (1, 4)))
    norm_gain = jnp.clip(1.0 + 0.18 * jax.random.normal(streams_of[1], (DMODEL,), jnp.float32), 0.1, 1.9)
    pool_proj = normal_values(streams_of[2], (DMODEL, POOL_WIDTH), DMODEL ** -0.5, 0.09375, ((0, 16), (1, 2)))
    query_proj = normal_values(streams_of[3], (DMODEL, RET_WIDTH), DMODEL ** -0.5, 0.09375, ((0, 16), (1, 2)))
    key_proj = normal_values(streams_of[4], (DMODEL, RET_WIDTH), DMODEL ** -0.5, 0.09375, ((0, 16), (1, 2)))
    value_proj = normal_values(streams_of[5], (DMODEL, RET_WIDTH), DMODEL ** -0.5, 0.09375, ((0, 16), (1, 2)))
    pool_map = normal_values(streams_of[6], (GROUPS, GROUP_DIM, GROUP_DIM), GROUP_DIM ** -0.5, 0.375)
    pool_scale = jnp.clip(1.0 + 0.18 * jax.random.normal(streams_of[7], (POOL_WIDTH,), jnp.float32), 0.1, 1.9)
    decay_rate = draw_decay_rate(jax.random.fold_in(streams_of[12], 71), 0)
    start_state = normal_values(streams_of[9], (SEQS, RET_HEADS, HEAD_DIM, HEAD_DIM), 16.0, 96.0, ((0, 4), (1, 2), (2, 4)), jnp.float32)
    pool_back = normal_values(streams_of[10], (POOL_WIDTH, DMODEL), (POOL_WIDTH + RET_WIDTH) ** -0.5, 0.125, ((0, 2), (1, 16)))
    retention_back = normal_values(streams_of[11], (RET_WIDTH, DMODEL), (POOL_WIDTH + RET_WIDTH) ** -0.5, 0.125, ((0, 2), (1, 16)))
    return {"tokens": tokens, "norm_gain": norm_gain, "pool_proj": pool_proj, "query_proj": query_proj, "key_proj": key_proj, "value_proj": value_proj, "pool_map": pool_map, "pool_scale": pool_scale, "decay_rate": decay_rate, "start_state": start_state, "pool_back": pool_back, "retention_back": retention_back}


eps = 1e-06
rope_base = 10000.0
highest_precision = lax.Precision.HIGHEST
window_list = (2, 4, 8, 16)

def rotate(values, positions):
    half_dim = values.shape[-1] // 2
    inv_freq = 1.0 / rope_base ** jnp.linspace(0.0, 1.0, half_dim, dtype=jnp.float32)
    angles = positions.astype(jnp.float32)[:, None] * inv_freq[None, :]
    cosine = jnp.cos(angles)[:, None, :]
    sine = jnp.sin(angles)[:, None, :]
    first_half = values[..., :half_dim]
    second_half = values[..., half_dim:]
    return jnp.concatenate([first_half * cosine - second_half * sine, first_half * sine + second_half * cosine], axis=-1)

def trailing_sums(extended, length):
    begin = extended.shape[0] - length
    running = extended[begin:]
    results = []
    for behind in range(1, 16):
        running = running + extended[begin - behind:begin - behind + length]
        if behind + 1 in window_list:
            results.append(running)
    return results

def reshape_blocks(array):
    return array.reshape((array.shape[0] // BLOCK, BLOCK) + array.shape[1:])

def block_retention(queries, keys_in, values_in, decay_rate, initial):
    length, head_count, head_dim = queries.shape
    within = jnp.arange(BLOCK, dtype=jnp.float32)
    distance = within[:, None] - within[None, :]
    decay_mask = jnp.where(distance[None] >= 0, jnp.exp(-jnp.maximum(distance, 0.0)[None] * decay_rate[:, None, None]), 0.0)
    query_decay_factor = jnp.exp(-(within + 1.0)[:, None] * decay_rate[None, :])
    key_decay_factor = jnp.exp(-(BLOCK - 1.0 - within)[:, None] * decay_rate[None, :])
    block_decay_factor = jnp.exp(-BLOCK * decay_rate)

    def advance(state_carry, inputs):
        block_queries, block_keys, block_values = inputs
        scores = jnp.einsum('ihk,jhk->hij', block_queries, block_keys, precision=highest_precision) * decay_mask
        inside = jnp.einsum('hij,jhv->ihv', scores, block_values, precision=highest_precision)
        across_blocks = jnp.einsum('bzy,zyx->bzx', block_queries * query_decay_factor[:, :, None], state_carry, precision=highest_precision)
        state_carry = state_carry * block_decay_factor[:, None, None] + jnp.einsum('flm,fld->lmd', block_keys * key_decay_factor[:, :, None], block_values, precision=highest_precision)
        return (state_carry, inside + across_blocks)
    final_state, outputs = lax.scan(advance, initial, (reshape_blocks(queries), reshape_blocks(keys_in), reshape_blocks(values_in)))
    return (outputs.reshape(length, head_count, values_in.shape[-1]), final_state)

def reference(tokens, norm_gain, pool_proj, query_proj, key_proj, value_proj, pool_map, pool_scale, decay_rate, start_state, pool_back, retention_back):
    weights_back = jnp.concatenate([pool_back, retention_back], axis=0)

    def one_sequence(operands):
        sequence, initial = operands
        floats = sequence.astype(jnp.float32)
        normed = (floats * lax.rsqrt(lax.optimization_barrier(jnp.mean(floats * floats, axis=-1, keepdims=True)) + eps) * norm_gain).astype(jnp.bfloat16)
        pool_in = jnp.dot(normed, pool_proj, preferred_element_type=jnp.float32).astype(jnp.bfloat16)
        query_bf = jnp.dot(normed, query_proj, preferred_element_type=jnp.float32).astype(jnp.bfloat16)
        key_bf = jnp.dot(normed, key_proj, preferred_element_type=jnp.float32).astype(jnp.bfloat16)
        value_bf = jnp.dot(normed, value_proj, preferred_element_type=jnp.float32).astype(jnp.bfloat16)
        positions = jnp.arange(SEQ_LEN, dtype=jnp.int32)
        extended = jnp.concatenate([jnp.zeros((HALO, POOL_WIDTH), jnp.float32), pool_in.astype(jnp.float32)], axis=0)
        sums_all = trailing_sums(extended, SEQ_LEN)
        pieces = []
        for group_idx in range(GROUPS):
            lower = group_idx * GROUP_DIM
            chosen = sums_all[group_idx][:, lower:lower + GROUP_DIM]
            counts = jnp.minimum(window_list[group_idx], positions + 1).astype(jnp.float32)
            inputs = extended[HALO:, lower:lower + GROUP_DIM]
            differ = (chosen / counts[:, None] - inputs).astype(jnp.bfloat16)
            pieces.append(jnp.dot(differ, pool_map[group_idx], preferred_element_type=jnp.float32))
        pool_out = (jnp.concatenate(pieces, axis=1) * pool_scale).astype(jnp.bfloat16)
        queries = rotate(query_bf.astype(jnp.float32).reshape(SEQ_LEN, RET_HEADS, HEAD_DIM), positions)
        keys_in = rotate(key_bf.astype(jnp.float32).reshape(SEQ_LEN, RET_HEADS, HEAD_DIM), positions) * HEAD_DIM ** (-0.5)
        values_in = value_bf.astype(jnp.float32).reshape(SEQ_LEN, RET_HEADS, HEAD_DIM)
        retained_output, final_state = block_retention(queries, keys_in, values_in, decay_rate, initial)
        retained_output = retained_output * lax.rsqrt(lax.optimization_barrier(jnp.mean(retained_output * retained_output, axis=-1, keepdims=True)) + eps)
        ret_out = retained_output.reshape(SEQ_LEN, RET_WIDTH).astype(jnp.bfloat16)
        joined = jnp.concatenate([pool_out, ret_out], axis=1)
        return jnp.dot(joined, weights_back, preferred_element_type=jnp.float32).astype(jnp.bfloat16)
    return lax.map(one_sequence, (tokens, start_state))
```

```python
import functools

from jax.experimental import pallas as pl
from jax.experimental.pallas import tpu as pltpu

import jax
import jax.numpy as jnp
from jax import lax
from jax.sharding import PartitionSpec as P

GROUPS = 4
BLOCK = 128
HALO = 16


eps = 1e-06
rope_base = 10000.0
highest_precision = lax.Precision.HIGHEST
window_list = (2, 4, 8, 16)


def shortened(x):
    return jax.tree.map(lambda a: a.astype(jnp.bfloat16) if a.dtype == jnp.float32 else a, x)


def shifted(x, axis, by):
    devices = lax.axis_size(axis)
    pairs = [(i, i + by) for i in range(devices) if 0 <= i + by < devices]
    return lax.ppermute(x, axis, pairs)


def carried_in(value, axis, join, neutral):
    count, mine = (lax.axis_size(axis), lax.axis_index(axis))
    pieces = jax.tree.map(lambda part: lax.all_gather(part, axis), value)
    running = jax.tree.map(
        lambda part, zero: jnp.full_like(part, 0) + jnp.asarray(zero, part.dtype), value, neutral
    )

    def turn(position, running):
        longer = join(running, jax.tree.map(lambda part: part[position], pieces))
        return jax.tree.map(lambda new, old: jnp.where(position < mine, new, old), longer, running)

    return lax.fori_loop(0, count - 1, turn, running)


def rotate(values, positions):
    half_dim = values.shape[-1] // 2
    inv_freq = 1.0 / rope_base ** jnp.linspace(0.0, 1.0, half_dim, dtype=jnp.float32)
    angles = positions.astype(jnp.float32)[:, None] * inv_freq[None, :]
    cosine = jnp.cos(angles)[:, None, :]
    sine = jnp.sin(angles)[:, None, :]
    first_half = values[..., :half_dim]
    second_half = values[..., half_dim:]
    return jnp.concatenate(
        [first_half * cosine - second_half * sine, first_half * sine + second_half * cosine],
        axis=-1,
    )


def trailing_sums(extended, length):
    begin = extended.shape[0] - length
    running = extended[begin:]
    results = []
    for behind in range(1, 16):
        running = running + extended[begin - behind : begin - behind + length]
        if behind + 1 in window_list:
            results.append(running)
    return results


def reshape_blocks(array):
    return array.reshape((array.shape[0] // BLOCK, BLOCK) + array.shape[1:])


def block_retention(queries, keys_in, values_in, decay_rate, initial):
    length, head_count, head_dim = queries.shape
    within = jnp.arange(BLOCK, dtype=jnp.float32)
    distance = within[:, None] - within[None, :]
    decay_mask = jnp.where(
        distance[None] >= 0,
        jnp.exp(-jnp.maximum(distance, 0.0)[None] * decay_rate[:, None, None]),
        0.0,
    )
    query_decay_factor = jnp.exp(-(within + 1.0)[:, None] * decay_rate[None, :])
    key_decay_factor = jnp.exp(-(BLOCK - 1.0 - within)[:, None] * decay_rate[None, :])
    block_decay_factor = jnp.exp(-BLOCK * decay_rate)

    def advance(state_carry, inputs):
        block_queries, block_keys, block_values = inputs
        scores = (
            jnp.einsum("ihk,jhk->hij", block_queries, block_keys, precision=highest_precision)
            * decay_mask
        )
        inside = jnp.einsum("hij,jhv->ihv", scores, block_values, precision=highest_precision)
        across_blocks = jnp.einsum(
            "bzy,zyx->bzx",
            block_queries * query_decay_factor[:, :, None],
            state_carry,
            precision=highest_precision,
        )
        state_carry = state_carry * block_decay_factor[:, None, None] + jnp.einsum(
            "flm,fld->lmd",
            block_keys * key_decay_factor[:, :, None],
            block_values,
            precision=highest_precision,
        )
        return (state_carry, inside + across_blocks)

    final_state, outputs = lax.scan(
        advance,
        initial,
        (reshape_blocks(queries), reshape_blocks(keys_in), reshape_blocks(values_in)),
    )
    return (outputs.reshape(length, head_count, values_in.shape[-1]), final_state)


def combine_states(earlier, latter):
    return (earlier[0] * latter[0], latter[0][:, None, None] * earlier[1] + latter[1])


def on_device(
    tokens,
    norm_gain,
    pool_proj,
    query_proj,
    key_proj,
    value_proj,
    pool_map,
    pool_scale,
    decay_rate,
    start_state,
    pool_back,
    retention_back,
):
    sequence = tokens[0]
    length = sequence.shape[0]
    tp_index = lax.axis_index("tp")
    sp_index = lax.axis_index("sp")
    tp_count = lax.axis_size("tp")
    floats = sequence.astype(jnp.float32)
    normed = (
        floats * lax.rsqrt(jnp.mean(floats * floats, axis=-1, keepdims=True) + eps) * norm_gain
    ).astype(jnp.bfloat16)
    group_normed = lax.all_gather(normed, "fs", axis=0, tiled=True)
    quarters = (
        lax.all_to_all(pool_proj, "fs", split_axis=1, concat_axis=0, tiled=True),
        lax.all_to_all(query_proj, "fs", split_axis=1, concat_axis=0, tiled=True),
        lax.all_to_all(key_proj, "fs", split_axis=1, concat_axis=0, tiled=True),
        lax.all_to_all(value_proj, "fs", split_axis=1, concat_axis=0, tiled=True),
    )
    pieces = (
        lax.all_gather(quarters[0], "sp", axis=0, tiled=True),
        lax.all_gather(quarters[1], "sp", axis=0, tiled=True),
        lax.all_gather(quarters[2], "sp", axis=0, tiled=True),
        lax.all_gather(quarters[3], "sp", axis=0, tiled=True),
    )
    partial_cols = tuple(
        (jnp.dot(group_normed, piece_w, preferred_element_type=jnp.float32) for piece_w in pieces)
    )
    rounded = tuple((result.astype(jnp.bfloat16) for result in partial_cols))
    pool_in, query_bf, key_bf, value_bf = jax.tree.map(
        lambda part, own: part.astype(own.dtype),
        lax.all_to_all(shortened(rounded), "fs", split_axis=0, concat_axis=1, tiled=True),
        rounded,
    )
    positions = jnp.arange(length, dtype=jnp.int32) + sp_index * length
    before = shifted(pool_in[length - HALO :], "sp", 1)
    extended = jnp.concatenate([before, pool_in], axis=0).astype(jnp.float32)
    stacked = jnp.stack(trailing_sums(extended, length))
    local_groups = GROUPS // tp_count
    channels = pool_in.shape[1]
    group_dim = channels // local_groups
    group_maps = lax.dynamic_slice_in_dim(pool_map, tp_index * local_groups, local_groups, 0)
    scales = lax.dynamic_slice_in_dim(pool_scale, tp_index * channels, channels, 0)
    windows = jnp.array(window_list, dtype=jnp.int32)
    pieces = []
    for group_idx in range(local_groups):
        chosen_group = tp_index * local_groups + group_idx
        lower = group_idx * group_dim
        chosen = lax.dynamic_index_in_dim(stacked, chosen_group, 0, keepdims=False)[
            :, lower : lower + group_dim
        ]
        counts = jnp.minimum(windows[chosen_group], positions + 1).astype(jnp.float32)
        inputs = extended[HALO:, lower : lower + group_dim]
        differ = (chosen / counts[:, None] - inputs).astype(jnp.bfloat16)
        pieces.append(jnp.dot(differ, group_maps[group_idx], preferred_element_type=jnp.float32))
    pool_out = (jnp.concatenate(pieces, axis=1) * scales).astype(jnp.bfloat16)
    head_count = decay_rate.shape[0]
    head_dim = query_bf.shape[1] // head_count
    queries = rotate(query_bf.astype(jnp.float32).reshape(length, head_count, head_dim), positions)
    keys_in = rotate(
        key_bf.astype(jnp.float32).reshape(length, head_count, head_dim), positions
    ) * head_dim ** (-0.5)
    values_in = value_bf.astype(jnp.float32).reshape(length, head_count, head_dim)
    zeros_state = jnp.zeros((head_count, head_dim, head_dim), jnp.float32)
    local_output, local_state = block_retention(
        queries, keys_in, values_in, decay_rate, zeros_state
    )
    span_decay = jnp.exp(-decay_rate * length)
    whole_start = lax.all_gather(start_state, "sp", axis=2, tiled=True)[0]
    span_factor, carried_over = carried_in(
        (span_decay, local_state), "sp", combine_states, (jnp.ones_like(span_decay), zeros_state)
    )
    offset_float = (sp_index * length).astype(jnp.float32)
    carried_over = carried_over + jnp.exp(-decay_rate * offset_float)[:, None, None] * whole_start
    steps_in = jnp.arange(length, dtype=jnp.float32) + 1.0
    query_rows_scaled = queries * jnp.exp(-steps_in[:, None] * decay_rate[None, :])[:, :, None]
    retained_output = local_output + jnp.einsum(
        "lpi,pib->lpb", query_rows_scaled, carried_over, precision=highest_precision
    )
    retained_output = retained_output * lax.rsqrt(
        jnp.mean(retained_output * retained_output, axis=-1, keepdims=True) + eps
    )
    ret_out = retained_output.reshape(length, head_count * head_dim).astype(jnp.bfloat16)
    pool_cols, retention_cols = (
        lax.all_gather(pool_back, ("sp", "fs"), axis=1, tiled=True),
        lax.all_gather(retention_back, ("sp", "fs"), axis=1, tiled=True),
    )
    weight_local = jnp.concatenate([pool_cols, retention_cols], axis=0)
    joined = jnp.concatenate([pool_out, ret_out], axis=1)
    mixed = lax.psum_scatter(
        jnp.dot(joined, weight_local, preferred_element_type=jnp.float32).astype(jnp.bfloat16),
        "tp",
        scatter_dimension=0,
        tiled=True,
    )
    return mixed[None]


MESH = pl.DeviceIdType.MESH


def where_am_i():
    sp, fs, tp = (lax.axis_index(name) for name in ("sp", "fs", "tp"))
    return sp, fs, tp, fs // 2, fs % 2


def remote(src, dst, send, recv, target):
    return pltpu.make_async_remote_copy(
        src_ref=src, dst_ref=dst, send_sem=send, recv_sem=recv, device_id=target, device_id_type=MESH
    )


def cols(index, size):
    return pl.ds(pl.multiple_of(index * size, size), size)


def project_kernel(
    tok, gain, wp, wq, wk, wv, state, pb, rb,
    joined, start, backs,
    xn, xg, wg, part, got,
    w_send, w_recv, w_local, x_send, x_recv, x_local, f_send, f_recv,
    s_send, s_recv, b_send, b_recv, b_local, p_send, p_recv, j_send, j_recv,
):
    sp, fs, tp, y, x = where_am_i()
    nsp, nfs = 4, 4
    span, width = tok.shape
    half = span // 2
    feats = width // nsp
    rows, group = wg.shape[2], wg.shape[3]
    mats = (wp, wq, wk, wv)
    partner = (sp, fs, 1 - tp)
    waits = []

    for d in range(1, nfs):
        to = lax.rem(fs + d, nfs)
        for m, mat in enumerate(mats):
            c = remote(
                mat.at[:, cols(to // 2, group)], wg.at[fs, m], w_send.at[d - 1, m],
                w_recv.at[fs, m], (sp, to, tp),
            )
            c.start()
            waits.append(c)
    own_w = []
    for m, mat in enumerate(mats):
        c = pltpu.make_async_copy(mat.at[:, cols(y, group)], wg.at[fs, m], w_local.at[m])
        c.start()
        own_w.append(c)
    for j in range(2):
        for h in range(2):
            to_sp, to_fs = 2 * y + tp, 2 * j + x
            rs = state.shape[1]
            dst = start.at[pl.ds(pl.multiple_of(sp * rs, rs), rs)]
            same = (to_sp == sp) & (to_fs == fs) & (tp == h)

            @pl.when(same)
            def _():
                pltpu.make_async_copy(state.at[j], dst, s_recv.at[sp]).start()

            @pl.when(jnp.logical_not(same))
            def _():
                remote(state.at[j], dst, s_send.at[2 * j + h], s_recv.at[sp], (to_sp, to_fs, h)).start()

    floats = tok[...].astype(jnp.float32)
    xn[...] = (
        floats * lax.rsqrt(jnp.mean(floats * floats, axis=-1, keepdims=True) + eps) * gain[...]
    ).astype(jnp.bfloat16)

    mine = pl.ds(pl.multiple_of(tp * half, half), half)
    moves = [(dz, dy) for dz in range(nsp) for dy in range(2) if dz or dy]
    for i, (dz, dy) in enumerate(moves):
        to_sp, to_y = lax.rem(sp + dz, nsp), lax.rem(y + dy, 2)
        c = remote(
            xn.at[mine, cols(to_sp, feats)], xg.at[y, sp, mine], x_send.at[i],
            x_recv.at[y, sp], (to_sp, 2 * to_y + x, tp),
        )
        c.start()
        waits.append(c)
    own_x = pltpu.make_async_copy(xn.at[:, cols(sp, feats)], xg.at[y, sp], x_local)
    own_x.start()

    forwards = []
    for i, (dz, dy) in enumerate(moves):
        fr_sp, fr_y = lax.rem(sp + nsp - dz, nsp), lax.rem(y + dy, 2)
        slot = xg.at[fr_y, fr_sp, mine]
        remote(slot, slot, x_send.at[i], x_recv.at[fr_y, fr_sp], partner).wait_recv()
        c = remote(slot, slot, f_send.at[i], f_recv.at[i], partner)
        c.start()
        forwards.append(c)

    own_b = []
    for b, back in enumerate((pb, rb)):
        c = pltpu.make_async_copy(back, backs.at[fs, b], b_local.at[b])
        c.start()
        own_b.append(c)
        for d in range(1, nfs):
            to = lax.rem(fs + d, nfs)
            c = remote(back, backs.at[fs, b], b_send.at[d - 1, b], b_recv.at[fs, b], (sp, to, tp))
            c.start()
            waits.append(c)

    own_x.wait()
    for c in own_w:
        c.wait()
    for c in forwards:
        c.wait()
    for d in range(1, nfs):
        fr = lax.rem(fs + nfs - d, nfs)
        for m, mat in enumerate(mats):
            remote(
                mat.at[:, cols(y, group)], wg.at[fr, m], w_send.at[d - 1, m], w_recv.at[fr, m], partner
            ).wait_recv()

    tall = 2 * span
    for s in range(2):
        for h in range(2):
            for m in range(4):
                acc = jnp.zeros((tall, group), jnp.float32)
                for f in range(nfs):
                    lhs = jnp.concatenate(
                        [xg[s, 2 * h + k, :, f * rows : (f + 1) * rows] for k in range(2)], axis=0
                    )
                    acc += jnp.dot(lhs, wg[f, m], preferred_element_type=jnp.float32)
                part[s, h, :, m * group : (m + 1) * group] = acc.astype(jnp.bfloat16)
            same = (2 * s + tp == sp) & (tp == h)

            @pl.when(same)
            def _():
                pltpu.make_async_copy(part.at[s, h], got.at[sp], p_recv.at[sp]).start()

            @pl.when(jnp.logical_not(same))
            def _():
                remote(
                    part.at[s, h], got.at[sp], p_send.at[2 * s + h], p_recv.at[sp], (2 * s + tp, fs, h)
                ).start()

    for k in range(nsp):
        remote(part.at[0, 0], got.at[k], p_send.at[0], p_recv.at[k], partner).wait_recv()
    total = got[0].astype(jnp.float32)
    for k in range(1, nsp):
        total += got[k].astype(jnp.float32)
    joined[tp] = total.astype(jnp.bfloat16)
    last = remote(joined.at[tp], joined.at[tp], j_send, j_recv, partner)
    last.start()
    last.wait_send()
    remote(joined.at[1 - tp], joined.at[1 - tp], j_send, j_recv, partner).wait_recv()

    for j in range(2):
        for h in range(2):
            to_sp, to_fs = 2 * y + tp, 2 * j + x
            same = (to_sp == sp) & (to_fs == fs) & (tp == h)

            @pl.when(jnp.logical_not(same))
            def _():
                remote(state.at[j], start.at[pl.ds(0, state.shape[1])], s_send.at[2 * j + h], s_recv.at[0], partner).wait_send()

            same_p = (2 * j + tp == sp) & (tp == h)

            @pl.when(jnp.logical_not(same_p))
            def _():
                remote(part.at[j, h], got.at[0], p_send.at[2 * j + h], p_recv.at[0], partner).wait_send()

    for k in range(nsp):
        rs = state.shape[1]
        slot = start.at[k * rs : (k + 1) * rs]
        remote(slot, slot, s_send.at[0], s_recv.at[k], partner).wait_recv()
    for b, back in enumerate((pb, rb)):
        own_b[b].wait()
        for d in range(1, nfs):
            fr = lax.rem(fs + nfs - d, nfs)
            remote(back, backs.at[fr, b], b_send.at[d - 1, b], b_recv.at[fr, b], partner).wait_recv()
    for c in waits:
        c.wait_send()


def output_kernel(
    yh, backs, out,
    yg, accs, give, take, done,
    y_send, y_recv, g_send, g_recv, o_send, o_recv, o_local,
):
    sp, fs, tp, y, x = where_am_i()
    nsp, nfs = 4, 4
    half, wide = yh.shape
    group = wide // 2
    block = backs.shape[3]
    few = out.shape[0]
    across = nfs * block
    partner = (sp, fs, 1 - tp)
    s, p = sp // 2, sp % 2
    for k in range(nsp):
        same = (sp == k) & (s == y) & (p == tp)

        @pl.when(same)
        def _():
            pltpu.make_async_copy(yh, yg.at[y, tp], y_recv.at[y, tp]).start()

        @pl.when(jnp.logical_not(same))
        def _():
            remote(yh, yg.at[y, tp], y_send.at[k], y_recv.at[y, tp], (k, 2 * s + x, p)).start()

    gives = []
    for h in range(2):
        for q in range(2):
            remote(yh, yg.at[q, h], y_send.at[0], y_recv.at[q, h], partner).wait_recv()
        for f in range(nfs):
            acc = jnp.zeros((half, block), jnp.float32)
            for q in range(2):
                for b in range(2):
                    acc += jnp.dot(
                        yg[q, h, :, b * group : (b + 1) * group],
                        backs[f, b, q * group : (q + 1) * group, :],
                        preferred_element_type=jnp.float32,
                    )
            accs[h * half : (h + 1) * half, f * block : (f + 1) * block] = acc
        for k in (2 * h, 2 * h + 1):
            off = pl.multiple_of(k * 2 * few + (1 - tp) * few, few)
            give[k] = accs[pl.ds(off, few), :].astype(jnp.bfloat16)
            c = remote(give.at[k], take.at[k], g_send.at[k], g_recv.at[k], partner)
            c.start()
            gives.append(c)
    for k in range(nsp):
        gives[k].wait()
        off = pl.multiple_of(k * 2 * few + tp * few, few)
        done[k] = (accs[pl.ds(off, few), :] + take[k].astype(jnp.float32)).astype(jnp.bfloat16)
        dst = out.at[:, cols(sp, across)]

        @pl.when(sp == k)
        def _():
            pltpu.make_async_copy(done.at[k], dst, o_recv.at[sp]).start()

        @pl.when(sp != k)
        def _():
            remote(done.at[k], dst, o_send.at[k], o_recv.at[sp], (k, fs, tp)).start()

    for k in range(nsp):
        remote(done.at[k], out.at[:, k * across : (k + 1) * across], o_send.at[k], o_recv.at[k], partner).wait_recv()

        @pl.when(sp != k)
        def _():
            remote(done.at[k], out.at[:, k * across : (k + 1) * across], o_send.at[k], o_recv.at[k], partner).wait_send()

        same = (sp == k) & (s == y) & (p == tp)

        @pl.when(jnp.logical_not(same))
        def _():
            remote(yh, yg.at[0, 0], y_send.at[k], y_recv.at[0, 0], partner).wait_send()


def turned(values, cosine, sine):
    half_dim = values.shape[-1] // 2
    a, b = values[:, :half_dim], values[:, half_dim:]
    return jnp.concatenate([a * cosine - b * sine, a * sine + b * cosine], axis=-1)


def angles_of(positions, half_dim):
    inv_freq = 1.0 / rope_base ** jnp.linspace(0.0, 1.0, half_dim, dtype=jnp.float32)
    angles = positions.astype(jnp.float32)[:, None] * inv_freq[None, :]
    return jnp.cos(angles), jnp.sin(angles)


def paired(
    tokens, norm_gain, pool_proj, query_proj, key_proj, value_proj, pool_map, pool_scale,
    decay_rate, start_state, pool_back, retention_back,
):
    bf, f32 = jnp.bfloat16, jnp.float32
    sp, fs, tp, y, x = where_am_i()
    nsp = lax.axis_size("sp")
    tok = tokens[0]
    span, width = tok.shape
    rows, two = pool_proj.shape
    group = two // 2
    length = nsp * span
    half = length // 2
    vm, hbm = pl.BlockSpec(memory_space=pltpu.VMEM), pl.BlockSpec(memory_space=pl.ANY)
    dma = pltpu.SemaphoreType.DMA
    rs = start_state.shape[2]
    joined, start, backs = pl.pallas_call(
        project_kernel,
        out_shape=(
            jax.ShapeDtypeStruct((2, half, 4 * group), bf),
            jax.ShapeDtypeStruct((nsp * rs, group), bf),
            jax.ShapeDtypeStruct((4, 2) + pool_back.shape, bf),
        ),
        in_specs=[vm, vm, hbm, hbm, hbm, hbm, hbm, hbm, hbm],
        out_specs=(vm, vm, vm),
        scratch_shapes=[
            pltpu.VMEM((span, width), bf),
            pltpu.VMEM((2, nsp, span, width // nsp), bf),
            pltpu.VMEM((4, 4, rows, group), bf),
            pltpu.VMEM((2, 2, half, 4 * group), bf),
            pltpu.VMEM((nsp, half, 4 * group), bf),
            dma((3, 4)), dma((4, 4)), dma((4,)), dma((7,)), dma((2, nsp)), dma,
            dma((7,)), dma((7,)), dma((4,)), dma((nsp,)), dma((3, 2)), dma((4, 2)), dma((2,)),
            dma((4,)), dma((nsp,)), dma, dma,
        ],
        compiler_params=pltpu.CompilerParams(has_side_effects=True, vmem_limit_bytes=48 * 2**20),
        name="project",
    )(
        tok, norm_gain[None, :], pool_proj, query_proj, key_proj, value_proj,
        start_state[0].astype(bf), pool_back, retention_back,
    )
    whole = joined.reshape(length, 4 * group)
    mine = joined[tp] if False else lax.dynamic_index_in_dim(joined, tp, 0, keepdims=False)
    head = 2 * (sp % 2) + y
    local = lax.dynamic_index_in_dim(decay_rate, y, 0, keepdims=False)
    other = lax.ppermute(decay_rate, "tp", [(0, 1), (1, 0)])
    rate = jnp.where(sp % 2 == tp, local, lax.dynamic_index_in_dim(other, y, 0, keepdims=False))
    every = jnp.arange(length, dtype=jnp.int32)
    position = tp * half + jnp.arange(half, dtype=jnp.int32)

    pool_all = jnp.concatenate([jnp.zeros((HALO, group), f32), whole[:, :group].astype(f32)], axis=0)
    extended = lax.dynamic_slice_in_dim(pool_all, tp * half, half + HALO, 0)
    sums = trailing_sums(extended, half)
    windows = jnp.array(window_list, dtype=jnp.int32)
    chosen = sums[0]
    for i in range(1, GROUPS):
        chosen = jnp.where(head == i, sums[i], chosen)
    counts = jnp.minimum(windows[head], position + 1).astype(f32)
    differ = (chosen / counts[:, None] - extended[HALO:]).astype(bf)
    this_map = lax.dynamic_index_in_dim(pool_map, head, 0, keepdims=False)
    scale = lax.dynamic_slice_in_dim(pool_scale, head * group, group, 0)
    pool_out = (jnp.dot(differ, this_map, preferred_element_type=f32) * scale).astype(bf)

    cosine, sine = angles_of(every, group // 2)
    my_cos = lax.dynamic_slice_in_dim(cosine, tp * half, half, 0)
    my_sin = lax.dynamic_slice_in_dim(sine, tp * half, half, 0)
    rq = turned(mine[:, group : 2 * group].astype(f32), my_cos, my_sin)
    rk = turned(whole[:, 2 * group : 3 * group].astype(f32), cosine, sine) * group ** (-0.5)
    value = whole[:, 3 * group :].astype(f32)
    gap = (position[:, None] - every[None, :]).astype(f32)
    mask = jnp.where(gap >= 0, jnp.exp(-jnp.maximum(gap, 0.0) * rate), 0.0)
    high = lax.Precision.HIGHEST
    scores = jnp.dot(rq, rk.T, precision=high) * mask
    fade = jnp.exp(-(position.astype(f32) + 1.0) * rate)
    ret = jnp.dot(scores, value, precision=high) + jnp.dot(
        rq * fade[:, None], start.astype(f32), precision=high
    )
    ret = ret * lax.rsqrt(jnp.mean(ret * ret, axis=-1, keepdims=True) + eps)
    yh = jnp.concatenate([pool_out, ret.astype(bf)], axis=1)

    few = span // 2
    return pl.pallas_call(
        output_kernel,
        out_shape=jax.ShapeDtypeStruct((few, width), bf),
        in_specs=[vm, vm],
        out_specs=vm,
        scratch_shapes=[
            pltpu.VMEM((2, 2, half, 2 * group), bf),
            pltpu.VMEM((length, 4 * pool_back.shape[1]), f32),
            pltpu.VMEM((nsp, few, 4 * pool_back.shape[1]), bf),
            pltpu.VMEM((nsp, few, 4 * pool_back.shape[1]), bf),
            pltpu.VMEM((nsp, few, 4 * pool_back.shape[1]), bf),
            dma((nsp,)), dma((2, 2)), dma((nsp,)), dma((nsp,)), dma((nsp,)), dma((nsp,)), dma,
        ],
        compiler_params=pltpu.CompilerParams(has_side_effects=True, vmem_limit_bytes=48 * 2**20),
        name="output",
    )(yh, backs)[None]


def solution(mesh):
    sizes = mesh.shape
    small = sizes["sp"] == 4 and sizes["fs"] == 4 and sizes["tp"] == 2
    placed = (
        P("fs", "sp", None),
        P(),
        P(("sp", "fs"), "tp"),
        P(("sp", "fs"), "tp"),
        P(("sp", "fs"), "tp"),
        P(("sp", "fs"), "tp"),
        P(),
        P(),
        P("tp"),
        P("fs", "tp", "sp", None),
        P("tp", ("sp", "fs")),
        P("tp", ("sp", "fs")),
    )
    return jax.shard_map(
        paired if small else on_device,
        mesh=mesh,
        in_specs=placed,
        out_specs=P("fs", ("sp", "tp"), None),
        check_vma=False,
    )
```

```python
import functools

from jax.experimental import pallas as pl
from jax.experimental.pallas import tpu as pltpu

import jax
import jax.numpy as jnp
from jax import lax
from jax.sharding import PartitionSpec as P

GROUPS = 4
BLOCK = 128
HALO = 16


eps = 1e-06
rope_base = 10000.0
highest_precision = lax.Precision.HIGHEST
window_list = (2, 4, 8, 16)


def shortened(x):
    return jax.tree.map(lambda a: a.astype(jnp.bfloat16) if a.dtype == jnp.float32 else a, x)


def shifted(x, axis, by):
    devices = lax.axis_size(axis)
    pairs = [(i, i + by) for i in range(devices) if 0 <= i + by < devices]
    return lax.ppermute(x, axis, pairs)


def carried_in(value, axis, join, neutral):
    count, mine = (lax.axis_size(axis), lax.axis_index(axis))
    pieces = jax.tree.map(lambda part: lax.all_gather(part, axis), value)
    running = jax.tree.map(
        lambda part, zero: jnp.full_like(part, 0) + jnp.asarray(zero, part.dtype), value, neutral
    )

    def turn(position, running):
        longer = join(running, jax.tree.map(lambda part: part[position], pieces))
        return jax.tree.map(lambda new, old: jnp.where(position < mine, new, old), longer, running)

    return lax.fori_loop(0, count - 1, turn, running)


def rotate(values, positions):
    half_dim = values.shape[-1] // 2
    inv_freq = 1.0 / rope_base ** jnp.linspace(0.0, 1.0, half_dim, dtype=jnp.float32)
    angles = positions.astype(jnp.float32)[:, None] * inv_freq[None, :]
    cosine = jnp.cos(angles)[:, None, :]
    sine = jnp.sin(angles)[:, None, :]
    first_half = values[..., :half_dim]
    second_half = values[..., half_dim:]
    return jnp.concatenate(
        [first_half * cosine - second_half * sine, first_half * sine + second_half * cosine],
        axis=-1,
    )


def trailing_sums(extended, length):
    begin = extended.shape[0] - length
    running = extended[begin:]
    results = []
    for behind in range(1, 16):
        running = running + extended[begin - behind : begin - behind + length]
        if behind + 1 in window_list:
            results.append(running)
    return results


def reshape_blocks(array):
    return array.reshape((array.shape[0] // BLOCK, BLOCK) + array.shape[1:])


def block_retention(queries, keys_in, values_in, decay_rate, initial):
    length, head_count, head_dim = queries.shape
    within = jnp.arange(BLOCK, dtype=jnp.float32)
    distance = within[:, None] - within[None, :]
    decay_mask = jnp.where(
        distance[None] >= 0,
        jnp.exp(-jnp.maximum(distance, 0.0)[None] * decay_rate[:, None, None]),
        0.0,
    )
    query_decay_factor = jnp.exp(-(within + 1.0)[:, None] * decay_rate[None, :])
    key_decay_factor = jnp.exp(-(BLOCK - 1.0 - within)[:, None] * decay_rate[None, :])
    block_decay_factor = jnp.exp(-BLOCK * decay_rate)

    def advance(state_carry, inputs):
        block_queries, block_keys, block_values = inputs
        scores = (
            jnp.einsum("ihk,jhk->hij", block_queries, block_keys, precision=highest_precision)
            * decay_mask
        )
        inside = jnp.einsum("hij,jhv->ihv", scores, block_values, precision=highest_precision)
        across_blocks = jnp.einsum(
            "bzy,zyx->bzx",
            block_queries * query_decay_factor[:, :, None],
            state_carry,
            precision=highest_precision,
        )
        state_carry = state_carry * block_decay_factor[:, None, None] + jnp.einsum(
            "flm,fld->lmd",
            block_keys * key_decay_factor[:, :, None],
            block_values,
            precision=highest_precision,
        )
        return (state_carry, inside + across_blocks)

    final_state, outputs = lax.scan(
        advance,
        initial,
        (reshape_blocks(queries), reshape_blocks(keys_in), reshape_blocks(values_in)),
    )
    return (outputs.reshape(length, head_count, values_in.shape[-1]), final_state)


def combine_states(earlier, latter):
    return (earlier[0] * latter[0], latter[0][:, None, None] * earlier[1] + latter[1])


def on_device(
    tokens,
    norm_gain,
    pool_proj,
    query_proj,
    key_proj,
    value_proj,
    pool_map,
    pool_scale,
    decay_rate,
    start_state,
    pool_back,
    retention_back,
):
    sequence = tokens[0]
    length = sequence.shape[0]
    tp_index = lax.axis_index("tp")
    sp_index = lax.axis_index("sp")
    tp_count = lax.axis_size("tp")
    floats = sequence.astype(jnp.float32)
    normed = (
        floats * lax.rsqrt(jnp.mean(floats * floats, axis=-1, keepdims=True) + eps) * norm_gain
    ).astype(jnp.bfloat16)
    group_normed = lax.all_gather(normed, "fs", axis=0, tiled=True)
    quarters = (
        lax.all_to_all(pool_proj, "fs", split_axis=1, concat_axis=0, tiled=True),
        lax.all_to_all(query_proj, "fs", split_axis=1, concat_axis=0, tiled=True),
        lax.all_to_all(key_proj, "fs", split_axis=1, concat_axis=0, tiled=True),
        lax.all_to_all(value_proj, "fs", split_axis=1, concat_axis=0, tiled=True),
    )
    pieces = (
        lax.all_gather(quarters[0], "sp", axis=0, tiled=True),
        lax.all_gather(quarters[1], "sp", axis=0, tiled=True),
        lax.all_gather(quarters[2], "sp", axis=0, tiled=True),
        lax.all_gather(quarters[3], "sp", axis=0, tiled=True),
    )
    partial_cols = tuple(
        (jnp.dot(group_normed, piece_w, preferred_element_type=jnp.float32) for piece_w in pieces)
    )
    rounded = tuple((result.astype(jnp.bfloat16) for result in partial_cols))
    pool_in, query_bf, key_bf, value_bf = jax.tree.map(
        lambda part, own: part.astype(own.dtype),
        lax.all_to_all(shortened(rounded), "fs", split_axis=0, concat_axis=1, tiled=True),
        rounded,
    )
    positions = jnp.arange(length, dtype=jnp.int32) + sp_index * length
    before = shifted(pool_in[length - HALO :], "sp", 1)
    extended = jnp.concatenate([before, pool_in], axis=0).astype(jnp.float32)
    stacked = jnp.stack(trailing_sums(extended, length))
    local_groups = GROUPS // tp_count
    channels = pool_in.shape[1]
    group_dim = channels // local_groups
    group_maps = lax.dynamic_slice_in_dim(pool_map, tp_index * local_groups, local_groups, 0)
    scales = lax.dynamic_slice_in_dim(pool_scale, tp_index * channels, channels, 0)
    windows = jnp.array(window_list, dtype=jnp.int32)
    pieces = []
    for group_idx in range(local_groups):
        chosen_group = tp_index * local_groups + group_idx
        lower = group_idx * group_dim
        chosen = lax.dynamic_index_in_dim(stacked, chosen_group, 0, keepdims=False)[
            :, lower : lower + group_dim
        ]
        counts = jnp.minimum(windows[chosen_group], positions + 1).astype(jnp.float32)
        inputs = extended[HALO:, lower : lower + group_dim]
        differ = (chosen / counts[:, None] - inputs).astype(jnp.bfloat16)
        pieces.append(jnp.dot(differ, group_maps[group_idx], preferred_element_type=jnp.float32))
    pool_out = (jnp.concatenate(pieces, axis=1) * scales).astype(jnp.bfloat16)
    head_count = decay_rate.shape[0]
    head_dim = query_bf.shape[1] // head_count
    queries = rotate(query_bf.astype(jnp.float32).reshape(length, head_count, head_dim), positions)
    keys_in = rotate(
        key_bf.astype(jnp.float32).reshape(length, head_count, head_dim), positions
    ) * head_dim ** (-0.5)
    values_in = value_bf.astype(jnp.float32).reshape(length, head_count, head_dim)
    zeros_state = jnp.zeros((head_count, head_dim, head_dim), jnp.float32)
    local_output, local_state = block_retention(
        queries, keys_in, values_in, decay_rate, zeros_state
    )
    span_decay = jnp.exp(-decay_rate * length)
    whole_start = lax.all_gather(start_state, "sp", axis=2, tiled=True)[0]
    span_factor, carried_over = carried_in(
        (span_decay, local_state), "sp", combine_states, (jnp.ones_like(span_decay), zeros_state)
    )
    offset_float = (sp_index * length).astype(jnp.float32)
    carried_over = carried_over + jnp.exp(-decay_rate * offset_float)[:, None, None] * whole_start
    steps_in = jnp.arange(length, dtype=jnp.float32) + 1.0
    query_rows_scaled = queries * jnp.exp(-steps_in[:, None] * decay_rate[None, :])[:, :, None]
    retained_output = local_output + jnp.einsum(
        "lpi,pib->lpb", query_rows_scaled, carried_over, precision=highest_precision
    )
    retained_output = retained_output * lax.rsqrt(
        jnp.mean(retained_output * retained_output, axis=-1, keepdims=True) + eps
    )
    ret_out = retained_output.reshape(length, head_count * head_dim).astype(jnp.bfloat16)
    pool_cols, retention_cols = (
        lax.all_gather(pool_back, ("sp", "fs"), axis=1, tiled=True),
        lax.all_gather(retention_back, ("sp", "fs"), axis=1, tiled=True),
    )
    weight_local = jnp.concatenate([pool_cols, retention_cols], axis=0)
    joined = jnp.concatenate([pool_out, ret_out], axis=1)
    mixed = lax.psum_scatter(
        jnp.dot(joined, weight_local, preferred_element_type=jnp.float32).astype(jnp.bfloat16),
        "tp",
        scatter_dimension=0,
        tiled=True,
    )
    return mixed[None]


MESH = pl.DeviceIdType.MESH


def where_am_i():
    sp, fs, tp = (lax.axis_index(name) for name in ("sp", "fs", "tp"))
    return sp, fs, tp, fs // 2, fs % 2


def remote(src, dst, send, recv, target):
    return pltpu.make_async_remote_copy(
        src_ref=src, dst_ref=dst, send_sem=send, recv_sem=recv, device_id=target, device_id_type=MESH
    )


def cols(index, size):
    return pl.ds(pl.multiple_of(index * size, size), size)


def project_kernel(
    tok, gain, wp, wq, wk, wv, state, pb, rb,
    joined, start, backs,
    xn, xg, wg, part, got,
    w_send, w_recv, w_local, x_send, x_recv, x_local, f_send, f_recv,
    s_send, s_recv, b_send, b_recv, b_local, p_send, p_recv, j_send, j_recv,
):
    sp, fs, tp, y, x = where_am_i()
    nsp, nfs = 4, 4
    span, width = tok.shape
    half = span // 2
    feats = width // nsp
    rows, group = wg.shape[2], wg.shape[3]
    mats = (wp, wq, wk, wv)
    partner = (sp, fs, 1 - tp)
    waits = []

    def send_mat(m):
        for d in (3, 1, 2):
            to = lax.rem(fs + d, nfs)
            c = remote(
                mats[m].at[:, cols(to // 2, group)], wg.at[m, fs], w_send.at[d - 1, m],
                w_recv.at[m, fs], (sp, to, tp),
            )
            c.start()
            waits.append(c)
        c = pltpu.make_async_copy(mats[m].at[:, cols(y, group)], wg.at[m, fs], w_local.at[m])
        c.start()
        return c

    own_w = [send_mat(0)]

    floats = tok[...].astype(jnp.float32)
    xn[...] = (
        floats * lax.rsqrt(jnp.mean(floats * floats, axis=-1, keepdims=True) + eps) * gain[...]
    ).astype(jnp.bfloat16)

    mine = pl.ds(pl.multiple_of(tp * half, half), half)

    def slot_of(from_y, from_sp):
        return xg.at[from_y, pl.ds(pl.multiple_of(from_sp * span + tp * half, half), half)]

    moves = [(2, 1), (1, 1), (3, 1), (0, 1), (2, 0), (1, 0), (3, 0)]
    for i, (dz, dy) in enumerate(moves):
        to_sp, to_y = lax.rem(sp + dz, nsp), lax.rem(y + dy, 2)
        c = remote(
            xn.at[mine, cols(to_sp, feats)], slot_of(y, sp), x_send.at[i],
            x_recv.at[y, sp], (to_sp, 2 * to_y + x, tp),
        )
        c.start()
        waits.append(c)
    own_x = pltpu.make_async_copy(
        xn.at[:, cols(sp, feats)], xg.at[y, pl.ds(pl.multiple_of(sp * span, span), span)], x_local
    )
    own_x.start()
    for m in range(1, 4):
        own_w.append(send_mat(m))
    for j in range(2):
        for h in range(2):
            to_sp, to_fs = 2 * y + tp, 2 * j + x
            rs = state.shape[1]
            dst = start.at[pl.ds(pl.multiple_of(sp * rs, rs), rs)]
            same = (to_sp == sp) & (to_fs == fs) & (tp == h)

            @pl.when(same)
            def _():
                pltpu.make_async_copy(state.at[j], dst, s_recv.at[sp]).start()

            @pl.when(jnp.logical_not(same))
            def _():
                remote(state.at[j], dst, s_send.at[2 * j + h], s_recv.at[sp], (to_sp, to_fs, h)).start()

    own_b = []
    for b, back in enumerate((pb, rb)):
        c = pltpu.make_async_copy(back, backs.at[fs, b], b_local.at[b])
        c.start()
        own_b.append(c)
        for d in (3, 1, 2):
            to = lax.rem(fs + d, nfs)
            c = remote(back, backs.at[fs, b], b_send.at[d - 1, b], b_recv.at[fs, b], (sp, to, tp))
            c.start()
            waits.append(c)

    forwards = []
    for i in (3, 5, 6, 4, 1, 2, 0):
        dz, dy = moves[i]
        fr_sp, fr_y = lax.rem(sp + nsp - dz, nsp), lax.rem(y + dy, 2)
        slot = slot_of(fr_y, fr_sp)
        remote(slot, slot, x_send.at[i], x_recv.at[fr_y, fr_sp], partner).wait_recv()
        c = remote(slot, slot, f_send.at[i], f_recv.at[i], partner)
        c.start()
        forwards.append(c)
    own_x.wait()
    for c in forwards:
        c.wait()

    tall = 2 * span
    for m in range(4):
        own_w[m].wait()
        for d in range(1, nfs):
            fr = lax.rem(fs + nfs - d, nfs)
            remote(
                mats[m].at[:, cols(y, group)], wg.at[m, fr], w_send.at[d - 1, m], w_recv.at[m, fr], partner
            ).wait_recv()
        for s in range(2):
            acc = jnp.zeros((2 * tall, group), jnp.float32)
            for f in range(nfs):
                acc += jnp.dot(
                    xg[s, :, f * rows : (f + 1) * rows], wg[m, f], preferred_element_type=jnp.float32
                )
            part[m, s] = acc.astype(jnp.bfloat16)
            for h in range(2):
                same = (2 * s + tp == sp) & (tp == h)
                src = part.at[m, s, h * tall : (h + 1) * tall]

                @pl.when(same)
                def _():
                    pltpu.make_async_copy(src, got.at[m, sp], p_recv.at[m, sp]).start()

                @pl.when(jnp.logical_not(same))
                def _():
                    remote(
                        src, got.at[m, sp], p_send.at[m, 2 * s + h], p_recv.at[m, sp], (2 * s + tp, fs, h)
                    ).start()

    here = pl.ds(pl.multiple_of(tp * tall, tall), tall)
    there = pl.ds(pl.multiple_of((1 - tp) * tall, tall), tall)
    lasts = []
    for m in range(4):
        for k in range(nsp):
            remote(got.at[m, k], got.at[m, k], p_send.at[0, 0], p_recv.at[m, k], partner).wait_recv()
        total = got[m, 0].astype(jnp.float32)
        for k in range(1, nsp):
            total += got[m, k].astype(jnp.float32)
        joined[m, here] = total.astype(jnp.bfloat16)
        c = remote(joined.at[m, here], joined.at[m, here], j_send.at[m], j_recv.at[m], partner)
        c.start()
        lasts.append(c)
    for m in range(4):
        lasts[m].wait_send()
        remote(joined.at[m, there], joined.at[m, there], j_send.at[m], j_recv.at[m], partner).wait_recv()

    for j in range(2):
        for h in range(2):
            to_sp, to_fs = 2 * y + tp, 2 * j + x
            same = (to_sp == sp) & (to_fs == fs) & (tp == h)

            @pl.when(jnp.logical_not(same))
            def _():
                remote(state.at[j], start.at[pl.ds(0, state.shape[1])], s_send.at[2 * j + h], s_recv.at[0], partner).wait_send()

            same_p = (2 * j + tp == sp) & (tp == h)

            @pl.when(jnp.logical_not(same_p))
            def _():
                for m in range(4):
                    remote(got.at[m, 0], got.at[m, 0], p_send.at[m, 2 * j + h], p_recv.at[m, 0], partner).wait_send()

    for k in range(nsp):
        rs = state.shape[1]
        slot = start.at[k * rs : (k + 1) * rs]
        remote(slot, slot, s_send.at[0], s_recv.at[k], partner).wait_recv()
    for b, back in enumerate((pb, rb)):
        own_b[b].wait()
        for d in range(1, nfs):
            fr = lax.rem(fs + nfs - d, nfs)
            remote(back, backs.at[fr, b], b_send.at[d - 1, b], b_recv.at[fr, b], partner).wait_recv()
    for c in waits:
        c.wait_send()


def output_kernel(
    yh, backs, out,
    yg, accs, give, take, done,
    y_send, y_recv, g_send, g_recv, o_send, o_recv, o_local,
):
    sp, fs, tp, y, x = where_am_i()
    nsp, nfs = 4, 4
    half, wide = yh.shape
    group = wide // 2
    block = backs.shape[3]
    few = out.shape[0]
    across = nfs * block
    partner = (sp, fs, 1 - tp)
    s, p = sp // 2, sp % 2
    for k in range(nsp):
        same = (sp == k) & (s == y) & (p == tp)

        @pl.when(same)
        def _():
            pltpu.make_async_copy(yh, yg.at[y, tp], y_recv.at[y, tp]).start()

        @pl.when(jnp.logical_not(same))
        def _():
            remote(yh, yg.at[y, tp], y_send.at[k], y_recv.at[y, tp], (k, 2 * s + x, p)).start()

    gives = []
    for h in range(2):
        for q in range(2):
            remote(yh, yg.at[q, h], y_send.at[0], y_recv.at[q, h], partner).wait_recv()
        for f in range(nfs):
            acc = jnp.zeros((half, block), jnp.float32)
            for q in range(2):
                for b in range(2):
                    acc += jnp.dot(
                        yg[q, h, :, b * group : (b + 1) * group],
                        backs[f, b, q * group : (q + 1) * group, :],
                        preferred_element_type=jnp.float32,
                    )
            accs[h * half : (h + 1) * half, f * block : (f + 1) * block] = acc
        for k in (2 * h, 2 * h + 1):
            off = pl.multiple_of(k * 2 * few + (1 - tp) * few, few)
            give[k] = accs[pl.ds(off, few), :].astype(jnp.bfloat16)
            c = remote(give.at[k], take.at[k], g_send.at[k], g_recv.at[k], partner)
            c.start()
            gives.append(c)
    for k in range(nsp):
        gives[k].wait()
        off = pl.multiple_of(k * 2 * few + tp * few, few)
        done[k] = (accs[pl.ds(off, few), :] + take[k].astype(jnp.float32)).astype(jnp.bfloat16)
        dst = out.at[:, cols(sp, across)]

        @pl.when(sp == k)
        def _():
            pltpu.make_async_copy(done.at[k], dst, o_recv.at[sp]).start()

        @pl.when(sp != k)
        def _():
            remote(done.at[k], dst, o_send.at[k], o_recv.at[sp], (k, fs, tp)).start()

    for k in range(nsp):
        remote(done.at[k], out.at[:, k * across : (k + 1) * across], o_send.at[k], o_recv.at[k], partner).wait_recv()

        @pl.when(sp != k)
        def _():
            remote(done.at[k], out.at[:, k * across : (k + 1) * across], o_send.at[k], o_recv.at[k], partner).wait_send()

        same = (sp == k) & (s == y) & (p == tp)

        @pl.when(jnp.logical_not(same))
        def _():
            remote(yh, yg.at[0, 0], y_send.at[k], y_recv.at[0, 0], partner).wait_send()


def turned(values, cosine, sine):
    half_dim = values.shape[-1] // 2
    a, b = values[:, :half_dim], values[:, half_dim:]
    return jnp.concatenate([a * cosine - b * sine, a * sine + b * cosine], axis=-1)


def angles_of(positions, half_dim):
    inv_freq = 1.0 / rope_base ** jnp.linspace(0.0, 1.0, half_dim, dtype=jnp.float32)
    angles = positions.astype(jnp.float32)[:, None] * inv_freq[None, :]
    return jnp.cos(angles), jnp.sin(angles)


def paired(
    tokens, norm_gain, pool_proj, query_proj, key_proj, value_proj, pool_map, pool_scale,
    decay_rate, start_state, pool_back, retention_back,
):
    bf, f32 = jnp.bfloat16, jnp.float32
    sp, fs, tp, y, x = where_am_i()
    nsp = lax.axis_size("sp")
    tok = tokens[0]
    span, width = tok.shape
    rows, two = pool_proj.shape
    group = two // 2
    length = nsp * span
    half = length // 2
    vm, hbm = pl.BlockSpec(memory_space=pltpu.VMEM), pl.BlockSpec(memory_space=pl.ANY)
    dma = pltpu.SemaphoreType.DMA
    rs = start_state.shape[2]
    joined, start, backs = pl.pallas_call(
        project_kernel,
        out_shape=(
            jax.ShapeDtypeStruct((4, length, group), bf),
            jax.ShapeDtypeStruct((nsp * rs, group), bf),
            jax.ShapeDtypeStruct((4, 2) + pool_back.shape, bf),
        ),
        in_specs=[vm, vm, hbm, hbm, hbm, hbm, hbm, hbm, hbm],
        out_specs=(vm, vm, vm),
        scratch_shapes=[
            pltpu.VMEM((span, width), bf),
            pltpu.VMEM((2, nsp * span, width // nsp), bf),
            pltpu.VMEM((4, 4, rows, group), bf),
            pltpu.VMEM((4, 2, length, group), bf),
            pltpu.VMEM((4, nsp, half, group), bf),
            dma((3, 4)), dma((4, 4)), dma((4,)), dma((7,)), dma((2, nsp)), dma,
            dma((7,)), dma((7,)), dma((4,)), dma((nsp,)), dma((3, 2)), dma((4, 2)), dma((2,)),
            dma((4, 4)), dma((4, nsp)), dma((4,)), dma((4,)),
        ],
        compiler_params=pltpu.CompilerParams(has_side_effects=True, vmem_limit_bytes=60 * 2**20),
        name="project",
    )(
        tok, norm_gain[None, :], pool_proj, query_proj, key_proj, value_proj,
        start_state[0].astype(bf), pool_back, retention_back,
    )
    mine = lax.dynamic_slice_in_dim(joined[1], tp * half, half, 0)
    head = 2 * (sp % 2) + y
    local = lax.dynamic_index_in_dim(decay_rate, y, 0, keepdims=False)
    other = lax.ppermute(decay_rate, "tp", [(0, 1), (1, 0)])
    rate = jnp.where(sp % 2 == tp, local, lax.dynamic_index_in_dim(other, y, 0, keepdims=False))
    every = jnp.arange(length, dtype=jnp.int32)
    position = tp * half + jnp.arange(half, dtype=jnp.int32)

    pool_all = jnp.concatenate([jnp.zeros((HALO, group), f32), joined[0].astype(f32)], axis=0)
    extended = lax.dynamic_slice_in_dim(pool_all, tp * half, half + HALO, 0)
    sums = trailing_sums(extended, half)
    windows = jnp.array(window_list, dtype=jnp.int32)
    chosen = sums[0]
    for i in range(1, GROUPS):
        chosen = jnp.where(head == i, sums[i], chosen)
    counts = jnp.minimum(windows[head], position + 1).astype(f32)
    differ = (chosen / counts[:, None] - extended[HALO:]).astype(bf)
    this_map = lax.dynamic_index_in_dim(pool_map, head, 0, keepdims=False)
    scale = lax.dynamic_slice_in_dim(pool_scale, head * group, group, 0)
    pool_out = (jnp.dot(differ, this_map, preferred_element_type=f32) * scale).astype(bf)

    cosine, sine = angles_of(every, group // 2)
    my_cos = lax.dynamic_slice_in_dim(cosine, tp * half, half, 0)
    my_sin = lax.dynamic_slice_in_dim(sine, tp * half, half, 0)
    rq = turned(mine.astype(f32), my_cos, my_sin)
    rk = turned(joined[2].astype(f32), cosine, sine) * group ** (-0.5)
    value = joined[3].astype(f32)
    gap = (position[:, None] - every[None, :]).astype(f32)
    mask = jnp.where(gap >= 0, jnp.exp(-jnp.maximum(gap, 0.0) * rate), 0.0)
    high = lax.Precision.HIGHEST
    scores = jnp.dot(rq, rk.T, precision=high) * mask
    fade = jnp.exp(-(position.astype(f32) + 1.0) * rate)
    ret = jnp.dot(scores, value, precision=high) + jnp.dot(
        rq * fade[:, None], start.astype(f32), precision=high
    )
    ret = ret * lax.rsqrt(jnp.mean(ret * ret, axis=-1, keepdims=True) + eps)
    yh = jnp.concatenate([pool_out, ret.astype(bf)], axis=1)

    few = span // 2
    return pl.pallas_call(
        output_kernel,
        out_shape=jax.ShapeDtypeStruct((few, width), bf),
        in_specs=[vm, vm],
        out_specs=vm,
        scratch_shapes=[
            pltpu.VMEM((2, 2, half, 2 * group), bf),
            pltpu.VMEM((length, 4 * pool_back.shape[1]), f32),
            pltpu.VMEM((nsp, few, 4 * pool_back.shape[1]), bf),
            pltpu.VMEM((nsp, few, 4 * pool_back.shape[1]), bf),
            pltpu.VMEM((nsp, few, 4 * pool_back.shape[1]), bf),
            dma((nsp,)), dma((2, 2)), dma((nsp,)), dma((nsp,)), dma((nsp,)), dma((nsp,)), dma,
        ],
        compiler_params=pltpu.CompilerParams(has_side_effects=True, vmem_limit_bytes=60 * 2**20),
        name="output",
    )(yh, backs)[None]


def solution(mesh):
    sizes = mesh.shape
    small = sizes["sp"] == 4 and sizes["fs"] == 4 and sizes["tp"] == 2
    placed = (
        P("fs", "sp", None),
        P(),
        P(("sp", "fs"), "tp"),
        P(("sp", "fs"), "tp"),
        P(("sp", "fs"), "tp"),
        P(("sp", "fs"), "tp"),
        P(),
        P(),
        P("tp"),
        P("fs", "tp", "sp", None),
        P("tp", ("sp", "fs")),
        P("tp", ("sp", "fs")),
    )
    return jax.shard_map(
        paired if small else on_device,
        mesh=mesh,
        in_specs=placed,
        out_specs=P("fs", ("sp", "tp"), None),
        check_vma=False,
    )
```

```python
import functools

from jax.experimental import pallas as pl
from jax.experimental.pallas import tpu as pltpu

import jax
import jax.numpy as jnp
from jax import lax
from jax.sharding import PartitionSpec as P

GROUPS = 4
BLOCK = 128
HALO = 16


eps = 1e-06
rope_base = 10000.0
highest_precision = lax.Precision.HIGHEST
window_list = (2, 4, 8, 16)


def shortened(x):
    return jax.tree.map(lambda a: a.astype(jnp.bfloat16) if a.dtype == jnp.float32 else a, x)


def shifted(x, axis, by):
    devices = lax.axis_size(axis)
    pairs = [(i, i + by) for i in range(devices) if 0 <= i + by < devices]
    return lax.ppermute(x, axis, pairs)


def carried_in(value, axis, join, neutral):
    count, mine = (lax.axis_size(axis), lax.axis_index(axis))
    pieces = jax.tree.map(lambda part: lax.all_gather(part, axis), value)
    running = jax.tree.map(
        lambda part, zero: jnp.full_like(part, 0) + jnp.asarray(zero, part.dtype), value, neutral
    )

    def turn(position, running):
        longer = join(running, jax.tree.map(lambda part: part[position], pieces))
        return jax.tree.map(lambda new, old: jnp.where(position < mine, new, old), longer, running)

    return lax.fori_loop(0, count - 1, turn, running)


def rotate(values, positions):
    half_dim = values.shape[-1] // 2
    inv_freq = 1.0 / rope_base ** jnp.linspace(0.0, 1.0, half_dim, dtype=jnp.float32)
    angles = positions.astype(jnp.float32)[:, None] * inv_freq[None, :]
    cosine = jnp.cos(angles)[:, None, :]
    sine = jnp.sin(angles)[:, None, :]
    first_half = values[..., :half_dim]
    second_half = values[..., half_dim:]
    return jnp.concatenate(
        [first_half * cosine - second_half * sine, first_half * sine + second_half * cosine],
        axis=-1,
    )


def trailing_sums(extended, length):
    begin = extended.shape[0] - length
    running = extended[begin:]
    results = []
    for behind in range(1, 16):
        running = running + extended[begin - behind : begin - behind + length]
        if behind + 1 in window_list:
            results.append(running)
    return results


def reshape_blocks(array):
    return array.reshape((array.shape[0] // BLOCK, BLOCK) + array.shape[1:])


def block_retention(queries, keys_in, values_in, decay_rate, initial):
    length, head_count, head_dim = queries.shape
    within = jnp.arange(BLOCK, dtype=jnp.float32)
    distance = within[:, None] - within[None, :]
    decay_mask = jnp.where(
        distance[None] >= 0,
        jnp.exp(-jnp.maximum(distance, 0.0)[None] * decay_rate[:, None, None]),
        0.0,
    )
    query_decay_factor = jnp.exp(-(within + 1.0)[:, None] * decay_rate[None, :])
    key_decay_factor = jnp.exp(-(BLOCK - 1.0 - within)[:, None] * decay_rate[None, :])
    block_decay_factor = jnp.exp(-BLOCK * decay_rate)

    def advance(state_carry, inputs):
        block_queries, block_keys, block_values = inputs
        scores = (
            jnp.einsum("ihk,jhk->hij", block_queries, block_keys, precision=highest_precision)
            * decay_mask
        )
        inside = jnp.einsum("hij,jhv->ihv", scores, block_values, precision=highest_precision)
        across_blocks = jnp.einsum(
            "bzy,zyx->bzx",
            block_queries * query_decay_factor[:, :, None],
            state_carry,
            precision=highest_precision,
        )
        state_carry = state_carry * block_decay_factor[:, None, None] + jnp.einsum(
            "flm,fld->lmd",
            block_keys * key_decay_factor[:, :, None],
            block_values,
            precision=highest_precision,
        )
        return (state_carry, inside + across_blocks)

    final_state, outputs = lax.scan(
        advance,
        initial,
        (reshape_blocks(queries), reshape_blocks(keys_in), reshape_blocks(values_in)),
    )
    return (outputs.reshape(length, head_count, values_in.shape[-1]), final_state)


def combine_states(earlier, latter):
    return (earlier[0] * latter[0], latter[0][:, None, None] * earlier[1] + latter[1])


def on_device(
    tokens,
    norm_gain,
    pool_proj,
    query_proj,
    key_proj,
    value_proj,
    pool_map,
    pool_scale,
    decay_rate,
    start_state,
    pool_back,
    retention_back,
):
    sequence = tokens[0]
    length = sequence.shape[0]
    tp_index = lax.axis_index("tp")
    sp_index = lax.axis_index("sp")
    tp_count = lax.axis_size("tp")
    floats = sequence.astype(jnp.float32)
    normed = (
        floats * lax.rsqrt(jnp.mean(floats * floats, axis=-1, keepdims=True) + eps) * norm_gain
    ).astype(jnp.bfloat16)
    group_normed = lax.all_gather(normed, "fs", axis=0, tiled=True)
    quarters = (
        lax.all_to_all(pool_proj, "fs", split_axis=1, concat_axis=0, tiled=True),
        lax.all_to_all(query_proj, "fs", split_axis=1, concat_axis=0, tiled=True),
        lax.all_to_all(key_proj, "fs", split_axis=1, concat_axis=0, tiled=True),
        lax.all_to_all(value_proj, "fs", split_axis=1, concat_axis=0, tiled=True),
    )
    pieces = (
        lax.all_gather(quarters[0], "sp", axis=0, tiled=True),
        lax.all_gather(quarters[1], "sp", axis=0, tiled=True),
        lax.all_gather(quarters[2], "sp", axis=0, tiled=True),
        lax.all_gather(quarters[3], "sp", axis=0, tiled=True),
    )
    partial_cols = tuple(
        (jnp.dot(group_normed, piece_w, preferred_element_type=jnp.float32) for piece_w in pieces)
    )
    rounded = tuple((result.astype(jnp.bfloat16) for result in partial_cols))
    pool_in, query_bf, key_bf, value_bf = jax.tree.map(
        lambda part, own: part.astype(own.dtype),
        lax.all_to_all(shortened(rounded), "fs", split_axis=0, concat_axis=1, tiled=True),
        rounded,
    )
    positions = jnp.arange(length, dtype=jnp.int32) + sp_index * length
    before = shifted(pool_in[length - HALO :], "sp", 1)
    extended = jnp.concatenate([before, pool_in], axis=0).astype(jnp.float32)
    stacked = jnp.stack(trailing_sums(extended, length))
    local_groups = GROUPS // tp_count
    channels = pool_in.shape[1]
    group_dim = channels // local_groups
    group_maps = lax.dynamic_slice_in_dim(pool_map, tp_index * local_groups, local_groups, 0)
    scales = lax.dynamic_slice_in_dim(pool_scale, tp_index * channels, channels, 0)
    windows = jnp.array(window_list, dtype=jnp.int32)
    pieces = []
    for group_idx in range(local_groups):
        chosen_group = tp_index * local_groups + group_idx
        lower = group_idx * group_dim
        chosen = lax.dynamic_index_in_dim(stacked, chosen_group, 0, keepdims=False)[
            :, lower : lower + group_dim
        ]
        counts = jnp.minimum(windows[chosen_group], positions + 1).astype(jnp.float32)
        inputs = extended[HALO:, lower : lower + group_dim]
        differ = (chosen / counts[:, None] - inputs).astype(jnp.bfloat16)
        pieces.append(jnp.dot(differ, group_maps[group_idx], preferred_element_type=jnp.float32))
    pool_out = (jnp.concatenate(pieces, axis=1) * scales).astype(jnp.bfloat16)
    head_count = decay_rate.shape[0]
    head_dim = query_bf.shape[1] // head_count
    queries = rotate(query_bf.astype(jnp.float32).reshape(length, head_count, head_dim), positions)
    keys_in = rotate(
        key_bf.astype(jnp.float32).reshape(length, head_count, head_dim), positions
    ) * head_dim ** (-0.5)
    values_in = value_bf.astype(jnp.float32).reshape(length, head_count, head_dim)
    zeros_state = jnp.zeros((head_count, head_dim, head_dim), jnp.float32)
    local_output, local_state = block_retention(
        queries, keys_in, values_in, decay_rate, zeros_state
    )
    span_decay = jnp.exp(-decay_rate * length)
    whole_start = lax.all_gather(start_state, "sp", axis=2, tiled=True)[0]
    span_factor, carried_over = carried_in(
        (span_decay, local_state), "sp", combine_states, (jnp.ones_like(span_decay), zeros_state)
    )
    offset_float = (sp_index * length).astype(jnp.float32)
    carried_over = carried_over + jnp.exp(-decay_rate * offset_float)[:, None, None] * whole_start
    steps_in = jnp.arange(length, dtype=jnp.float32) + 1.0
    query_rows_scaled = queries * jnp.exp(-steps_in[:, None] * decay_rate[None, :])[:, :, None]
    retained_output = local_output + jnp.einsum(
        "lpi,pib->lpb", query_rows_scaled, carried_over, precision=highest_precision
    )
    retained_output = retained_output * lax.rsqrt(
        jnp.mean(retained_output * retained_output, axis=-1, keepdims=True) + eps
    )
    ret_out = retained_output.reshape(length, head_count * head_dim).astype(jnp.bfloat16)
    pool_cols, retention_cols = (
        lax.all_gather(pool_back, ("sp", "fs"), axis=1, tiled=True),
        lax.all_gather(retention_back, ("sp", "fs"), axis=1, tiled=True),
    )
    weight_local = jnp.concatenate([pool_cols, retention_cols], axis=0)
    joined = jnp.concatenate([pool_out, ret_out], axis=1)
    mixed = lax.psum_scatter(
        jnp.dot(joined, weight_local, preferred_element_type=jnp.float32).astype(jnp.bfloat16),
        "tp",
        scatter_dimension=0,
        tiled=True,
    )
    return mixed[None]


MESH = pl.DeviceIdType.MESH


def where_am_i():
    sp, fs, tp = (lax.axis_index(name) for name in ("sp", "fs", "tp"))
    return sp, fs, tp, fs // 2, fs % 2


def remote(src, dst, send, recv, target):
    return pltpu.make_async_remote_copy(
        src_ref=src, dst_ref=dst, send_sem=send, recv_sem=recv, device_id=target, device_id_type=MESH
    )


def greet(others):
    barrier = pltpu.get_barrier_semaphore()
    for other in others:
        pl.semaphore_signal(barrier, inc=1, device_id=other, device_id_type=MESH)
    pl.semaphore_wait(barrier, len(others))


def cols(index, size):
    return pl.ds(pl.multiple_of(index * size, size), size)


def project_kernel(
    tok, gain, wp, wq, wk, wv, state, pb, rb,
    joined, start, backs,
    xn, xg, wg, part, got,
    w_send, w_recv, w_local, x_send, x_recv, x_local, f_send, f_recv,
    s_send, s_recv, b_send, b_recv, b_local, p_send, p_recv, j_send, j_recv,
):
    sp, fs, tp, y, x = where_am_i()
    nsp, nfs = 4, 4
    span, width = tok.shape
    half = span // 2
    feats = width // nsp
    rows, group = wg.shape[2], wg.shape[3]
    mats = (wp, wq, wk, wv)
    partner = (sp, fs, 1 - tp)
    waits = []
    greet(
        [
            (lax.rem(sp + dz, nsp), 2 * lax.rem(y + dy, 2) + x, lax.rem(tp + dt, 2))
            for dz in range(nsp) for dy in range(2) for dt in range(2) if dz or dy or dt
        ]
        + [(sp, 2 * lax.rem(y + dy, 2) + 1 - x, tp) for dy in range(2)]
    )

    def send_mat(m):
        for d in (3, 1, 2):
            to = lax.rem(fs + d, nfs)
            c = remote(
                mats[m].at[:, cols(to // 2, group)], wg.at[m, fs], w_send.at[d - 1, m],
                w_recv.at[m, fs], (sp, to, tp),
            )
            c.start()
            waits.append(c)
        c = pltpu.make_async_copy(mats[m].at[:, cols(y, group)], wg.at[m, fs], w_local.at[m])
        c.start()
        return c

    own_w = [send_mat(0)]

    floats = tok[...].astype(jnp.float32)
    xn[...] = (
        floats * lax.rsqrt(jnp.mean(floats * floats, axis=-1, keepdims=True) + eps) * gain[...]
    ).astype(jnp.bfloat16)

    mine = pl.ds(pl.multiple_of(tp * half, half), half)

    def slot_of(from_y, from_sp):
        return xg.at[from_y, pl.ds(pl.multiple_of(from_sp * span + tp * half, half), half)]

    peer = (sp, 2 * (1 - y) + x, tp)
    for dz in (2, 1, 3, 0):
        to_sp = lax.rem(sp + dz, nsp)
        c = remote(
            xn.at[mine, cols(to_sp, feats)], slot_of(y, sp), x_send.at[dz], x_recv.at[y, sp],
            (to_sp, fs, tp) if dz else peer,
        )
        c.start()
        waits.append(c)
    own_x = pltpu.make_async_copy(
        xn.at[:, cols(sp, feats)], xg.at[y, pl.ds(pl.multiple_of(sp * span, span), span)], x_local
    )
    own_x.start()
    for m in range(1, 4):
        own_w.append(send_mat(m))
    for j in range(2):
        for h in range(2):
            to_sp, to_fs = 2 * y + tp, 2 * j + x
            rs = state.shape[1]
            dst = start.at[pl.ds(pl.multiple_of(sp * rs, rs), rs)]
            same = (to_sp == sp) & (to_fs == fs) & (tp == h)

            @pl.when(same)
            def _():
                pltpu.make_async_copy(state.at[j], dst, s_recv.at[sp]).start()

            @pl.when(jnp.logical_not(same))
            def _():
                remote(state.at[j], dst, s_send.at[2 * j + h], s_recv.at[sp], (to_sp, to_fs, h)).start()

    own_b = []
    for b, back in enumerate((pb, rb)):
        c = pltpu.make_async_copy(back, backs.at[fs, b], b_local.at[b])
        c.start()
        own_b.append(c)
        for d in (3, 1, 2):
            to = lax.rem(fs + d, nfs)
            c = remote(back, backs.at[fs, b], b_send.at[d - 1, b], b_recv.at[fs, b], (sp, to, tp))
            c.start()
            waits.append(c)

    forwards = []

    def arrived(from_y, from_sp, order):
        slot = slot_of(from_y, from_sp)
        remote(slot, slot, x_send.at[0], x_recv.at[from_y, from_sp], partner).wait_recv()
        c = remote(slot, slot, f_send.at[order], f_recv.at[order], partner)
        c.start()
        forwards.append(c)
        return slot

    for dz in (1, 3, 2):
        fr_sp = lax.rem(sp + nsp - dz, nsp)
        slot = arrived(y, fr_sp, dz - 1)
        c = remote(slot, slot, x_send.at[nsp + dz - 1], x_recv.at[y, fr_sp], peer)
        c.start()
        waits.append(c)
    for dz in (0, 1, 3, 2):
        arrived(1 - y, lax.rem(sp + nsp - dz, nsp), 3 + dz)
    own_x.wait()
    for c in forwards:
        c.wait()

    tall = 2 * span
    for m in range(4):
        own_w[m].wait()
        for d in range(1, nfs):
            fr = lax.rem(fs + nfs - d, nfs)
            remote(
                mats[m].at[:, cols(y, group)], wg.at[m, fr], w_send.at[d - 1, m], w_recv.at[m, fr], partner
            ).wait_recv()
        for s in range(2):
            acc = jnp.zeros((2 * tall, group), jnp.float32)
            for f in range(nfs):
                acc += jnp.dot(
                    xg[s, :, f * rows : (f + 1) * rows], wg[m, f], preferred_element_type=jnp.float32
                )
            part[m, s] = acc.astype(jnp.bfloat16)
            for h in range(2):
                same = (2 * s + tp == sp) & (tp == h)
                src = part.at[m, s, h * tall : (h + 1) * tall]

                @pl.when(same)
                def _():
                    pltpu.make_async_copy(src, got.at[m, sp], p_recv.at[m, sp]).start()

                @pl.when(jnp.logical_not(same))
                def _():
                    remote(
                        src, got.at[m, sp], p_send.at[m, 2 * s + h], p_recv.at[m, sp], (2 * s + tp, fs, h)
                    ).start()

    here = pl.ds(pl.multiple_of(tp * tall, tall), tall)
    there = pl.ds(pl.multiple_of((1 - tp) * tall, tall), tall)
    lasts = []
    for m in range(4):
        for k in range(nsp):
            remote(got.at[m, k], got.at[m, k], p_send.at[0, 0], p_recv.at[m, k], partner).wait_recv()
        total = got[m, 0].astype(jnp.float32)
        for k in range(1, nsp):
            total += got[m, k].astype(jnp.float32)
        joined[m, here] = total.astype(jnp.bfloat16)
        c = remote(joined.at[m, here], joined.at[m, here], j_send.at[m], j_recv.at[m], partner)
        c.start()
        lasts.append(c)
    for m in range(4):
        lasts[m].wait_send()
        remote(joined.at[m, there], joined.at[m, there], j_send.at[m], j_recv.at[m], partner).wait_recv()

    for j in range(2):
        for h in range(2):
            to_sp, to_fs = 2 * y + tp, 2 * j + x
            same = (to_sp == sp) & (to_fs == fs) & (tp == h)

            @pl.when(jnp.logical_not(same))
            def _():
                remote(state.at[j], start.at[pl.ds(0, state.shape[1])], s_send.at[2 * j + h], s_recv.at[0], partner).wait_send()

            same_p = (2 * j + tp == sp) & (tp == h)

            @pl.when(jnp.logical_not(same_p))
            def _():
                for m in range(4):
                    remote(got.at[m, 0], got.at[m, 0], p_send.at[m, 2 * j + h], p_recv.at[m, 0], partner).wait_send()

    for k in range(nsp):
        rs = state.shape[1]
        slot = start.at[k * rs : (k + 1) * rs]
        remote(slot, slot, s_send.at[0], s_recv.at[k], partner).wait_recv()
    for b, back in enumerate((pb, rb)):
        own_b[b].wait()
        for d in range(1, nfs):
            fr = lax.rem(fs + nfs - d, nfs)
            remote(back, backs.at[fr, b], b_send.at[d - 1, b], b_recv.at[fr, b], partner).wait_recv()
    for c in waits:
        c.wait_send()


def output_kernel(
    yh, backs, out,
    yg, stage, accs, give, take, done,
    y_send, y_recv, t_send, t_recv, g_send, g_recv, o_send, o_recv,
):
    sp, fs, tp, y, x = where_am_i()
    nsp, nfs = 4, 4
    half, wide = yh.shape
    group = wide // 2
    block = backs.shape[3]
    few = out.shape[0]
    across = nfs * block
    partner = (sp, fs, 1 - tp)
    s, p = sp // 2, sp % 2
    peer = (sp, 2 * (1 - y) + x, tp)
    greet(
        [
            (lax.rem(sp + dz, nsp), fs, lax.rem(tp + dt, 2))
            for dz in range(nsp) for dt in range(2) if dz or dt
        ]
        + [peer]
    )
    for dz in (2, 1, 3, 0):
        k = lax.rem(sp + dz, nsp)
        for staged, dst, sem in ((False, yg.at[y, tp], y_recv.at[y, tp]), (True, stage.at[tp], t_recv.at[tp])):
            kind = (s != y) if staged else (s == y)
            if dz:

                @pl.when(kind)
                def _():
                    remote(yh, dst, y_send.at[dz], sem, (k, fs, p)).start()
            else:

                @pl.when(kind & (p == tp))
                def _():
                    pltpu.make_async_copy(yh, dst, sem).start()

                @pl.when(kind & (p != tp))
                def _():
                    remote(yh, dst, y_send.at[dz], sem, partner).start()

    passed = []
    for h in range(2):
        remote(yh, stage.at[h], y_send.at[0], t_recv.at[h], partner).wait_recv()
        c = remote(stage.at[h], yg.at[y, h], t_send.at[h], y_recv.at[y, h], peer)
        c.start()
        passed.append(c)
    gives = []
    for h in range(2):
        for q in range(2):
            remote(yh, yg.at[q, h], y_send.at[0], y_recv.at[q, h], partner).wait_recv()
        for f in range(nfs):
            acc = jnp.zeros((half, block), jnp.float32)
            for q in range(2):
                for b in range(2):
                    acc += jnp.dot(
                        yg[q, h, :, b * group : (b + 1) * group],
                        backs[f, b, q * group : (q + 1) * group, :],
                        preferred_element_type=jnp.float32,
                    )
            accs[h * half : (h + 1) * half, f * block : (f + 1) * block] = acc
        for k in (2 * h, 2 * h + 1):
            off = pl.multiple_of(k * 2 * few + (1 - tp) * few, few)
            give[k] = accs[pl.ds(off, few), :].astype(jnp.bfloat16)
            c = remote(give.at[k], take.at[k], g_send.at[k], g_recv.at[k], partner)
            c.start()
            gives.append(c)
    for k in range(nsp):
        gives[k].wait()
        off = pl.multiple_of(k * 2 * few + tp * few, few)
        done[k] = (accs[pl.ds(off, few), :] + take[k].astype(jnp.float32)).astype(jnp.bfloat16)
        dst = out.at[:, cols(sp, across)]

        @pl.when(sp == k)
        def _():
            pltpu.make_async_copy(done.at[k], dst, o_recv.at[sp]).start()

        @pl.when(sp != k)
        def _():
            remote(done.at[k], dst, o_send.at[k], o_recv.at[sp], (k, fs, tp)).start()

    for k in range(nsp):
        remote(done.at[k], out.at[:, k * across : (k + 1) * across], o_send.at[k], o_recv.at[k], partner).wait_recv()

        @pl.when(sp != k)
        def _():
            remote(done.at[k], out.at[:, k * across : (k + 1) * across], o_send.at[k], o_recv.at[k], partner).wait_send()

    for dz in range(1, nsp):
        remote(yh, yg.at[0, 0], y_send.at[dz], y_recv.at[0, 0], partner).wait_send()

    @pl.when(p != tp)
    def _():
        remote(yh, yg.at[0, 0], y_send.at[0], y_recv.at[0, 0], partner).wait_send()

    for c in passed:
        c.wait_send()


def turned(values, cosine, sine):
    half_dim = values.shape[-1] // 2
    a, b = values[:, :half_dim], values[:, half_dim:]
    return jnp.concatenate([a * cosine - b * sine, a * sine + b * cosine], axis=-1)


def angles_of(positions, half_dim):
    inv_freq = 1.0 / rope_base ** jnp.linspace(0.0, 1.0, half_dim, dtype=jnp.float32)
    angles = positions.astype(jnp.float32)[:, None] * inv_freq[None, :]
    return jnp.cos(angles), jnp.sin(angles)


def paired(
    tokens, norm_gain, pool_proj, query_proj, key_proj, value_proj, pool_map, pool_scale,
    decay_rate, start_state, pool_back, retention_back,
):
    bf, f32 = jnp.bfloat16, jnp.float32
    sp, fs, tp, y, x = where_am_i()
    nsp = lax.axis_size("sp")
    tok = tokens[0]
    span, width = tok.shape
    rows, two = pool_proj.shape
    group = two // 2
    length = nsp * span
    half = length // 2
    vm, hbm = pl.BlockSpec(memory_space=pltpu.VMEM), pl.BlockSpec(memory_space=pl.ANY)
    dma = pltpu.SemaphoreType.DMA
    rs = start_state.shape[2]
    joined, start, backs = pl.pallas_call(
        project_kernel,
        out_shape=(
            jax.ShapeDtypeStruct((4, length, group), bf),
            jax.ShapeDtypeStruct((nsp * rs, group), bf),
            jax.ShapeDtypeStruct((4, 2) + pool_back.shape, bf),
        ),
        in_specs=[vm, vm, hbm, hbm, hbm, hbm, hbm, hbm, hbm],
        out_specs=(vm, vm, vm),
        scratch_shapes=[
            pltpu.VMEM((span, width), bf),
            pltpu.VMEM((2, nsp * span, width // nsp), bf),
            pltpu.VMEM((4, 4, rows, group), bf),
            pltpu.VMEM((4, 2, length, group), bf),
            pltpu.VMEM((4, nsp, half, group), bf),
            dma((3, 4)), dma((4, 4)), dma((4,)), dma((7,)), dma((2, nsp)), dma,
            dma((7,)), dma((7,)), dma((4,)), dma((nsp,)), dma((3, 2)), dma((4, 2)), dma((2,)),
            dma((4, 4)), dma((4, nsp)), dma((4,)), dma((4,)),
        ],
        compiler_params=pltpu.CompilerParams(collective_id=0, has_side_effects=True, vmem_limit_bytes=60 * 2**20),
        name="project",
    )(
        tok, norm_gain[None, :], pool_proj, query_proj, key_proj, value_proj,
        start_state[0].astype(bf), pool_back, retention_back,
    )
    mine = lax.dynamic_slice_in_dim(joined[1], tp * half, half, 0)
    head = 2 * (sp % 2) + y
    local = lax.dynamic_index_in_dim(decay_rate, y, 0, keepdims=False)
    other = lax.ppermute(decay_rate, "tp", [(0, 1), (1, 0)])
    rate = jnp.where(sp % 2 == tp, local, lax.dynamic_index_in_dim(other, y, 0, keepdims=False))
    every = jnp.arange(length, dtype=jnp.int32)
    position = tp * half + jnp.arange(half, dtype=jnp.int32)

    pool_all = jnp.concatenate([jnp.zeros((HALO, group), f32), joined[0].astype(f32)], axis=0)
    extended = lax.dynamic_slice_in_dim(pool_all, tp * half, half + HALO, 0)
    sums = trailing_sums(extended, half)
    windows = jnp.array(window_list, dtype=jnp.int32)
    chosen = sums[0]
    for i in range(1, GROUPS):
        chosen = jnp.where(head == i, sums[i], chosen)
    counts = jnp.minimum(windows[head], position + 1).astype(f32)
    differ = (chosen / counts[:, None] - extended[HALO:]).astype(bf)
    this_map = lax.dynamic_index_in_dim(pool_map, head, 0, keepdims=False)
    scale = lax.dynamic_slice_in_dim(pool_scale, head * group, group, 0)
    pool_out = (jnp.dot(differ, this_map, preferred_element_type=f32) * scale).astype(bf)

    cosine, sine = angles_of(every, group // 2)
    my_cos = lax.dynamic_slice_in_dim(cosine, tp * half, half, 0)
    my_sin = lax.dynamic_slice_in_dim(sine, tp * half, half, 0)
    rq = turned(mine.astype(f32), my_cos, my_sin)
    rk = turned(joined[2].astype(f32), cosine, sine) * group ** (-0.5)
    value = joined[3].astype(f32)
    gap = (position[:, None] - every[None, :]).astype(f32)
    mask = jnp.where(gap >= 0, jnp.exp(-jnp.maximum(gap, 0.0) * rate), 0.0)
    high = lax.Precision.HIGHEST
    scores = jnp.dot(rq, rk.T, precision=high) * mask
    fade = jnp.exp(-(position.astype(f32) + 1.0) * rate)
    ret = jnp.dot(scores, value, precision=high) + jnp.dot(
        rq * fade[:, None], start.astype(f32), precision=high
    )
    ret = ret * lax.rsqrt(jnp.mean(ret * ret, axis=-1, keepdims=True) + eps)
    yh = jnp.concatenate([pool_out, ret.astype(bf)], axis=1)

    few = span // 2
    return pl.pallas_call(
        output_kernel,
        out_shape=jax.ShapeDtypeStruct((few, width), bf),
        in_specs=[vm, vm],
        out_specs=vm,
        scratch_shapes=[
            pltpu.VMEM((2, 2, half, 2 * group), bf),
            pltpu.VMEM((2, half, 2 * group), bf),
            pltpu.VMEM((length, 4 * pool_back.shape[1]), f32),
            pltpu.VMEM((nsp, few, 4 * pool_back.shape[1]), bf),
            pltpu.VMEM((nsp, few, 4 * pool_back.shape[1]), bf),
            pltpu.VMEM((nsp, few, 4 * pool_back.shape[1]), bf),
            dma((nsp,)), dma((2, 2)), dma((2,)), dma((2,)), dma((nsp,)), dma((nsp,)), dma((nsp,)), dma((nsp,)),
        ],
        compiler_params=pltpu.CompilerParams(collective_id=1, has_side_effects=True, vmem_limit_bytes=60 * 2**20),
        name="output",
    )(yh, backs)[None]


def solution(mesh):
    sizes = mesh.shape
    small = sizes["sp"] == 4 and sizes["fs"] == 4 and sizes["tp"] == 2
    placed = (
        P("fs", "sp", None),
        P(),
        P(("sp", "fs"), "tp"),
        P(("sp", "fs"), "tp"),
        P(("sp", "fs"), "tp"),
        P(("sp", "fs"), "tp"),
        P(),
        P(),
        P("tp"),
        P("fs", "tp", "sp", None),
        P("tp", ("sp", "fs")),
        P("tp", ("sp", "fs")),
    )
    return jax.shard_map(
        paired if small else on_device,
        mesh=mesh,
        in_specs=placed,
        out_specs=P("fs", ("sp", "tp"), None),
        check_vma=False,
    )
```

```python
import functools

from jax.experimental import pallas as pl
from jax.experimental.pallas import tpu as pltpu

import jax
import jax.numpy as jnp
from jax import lax
from jax.sharding import PartitionSpec as P

GROUPS = 4
BLOCK = 128
HALO = 16


eps = 1e-06
rope_base = 10000.0
highest_precision = lax.Precision.HIGHEST
window_list = (2, 4, 8, 16)


def shortened(x):
    return jax.tree.map(lambda a: a.astype(jnp.bfloat16) if a.dtype == jnp.float32 else a, x)


def shifted(x, axis, by):
    devices = lax.axis_size(axis)
    pairs = [(i, i + by) for i in range(devices) if 0 <= i + by < devices]
    return lax.ppermute(x, axis, pairs)


def carried_in(value, axis, join, neutral):
    count, mine = (lax.axis_size(axis), lax.axis_index(axis))
    pieces = jax.tree.map(lambda part: lax.all_gather(part, axis), value)
    running = jax.tree.map(
        lambda part, zero: jnp.full_like(part, 0) + jnp.asarray(zero, part.dtype), value, neutral
    )

    def turn(position, running):
        longer = join(running, jax.tree.map(lambda part: part[position], pieces))
        return jax.tree.map(lambda new, old: jnp.where(position < mine, new, old), longer, running)

    return lax.fori_loop(0, count - 1, turn, running)


def rotate(values, positions):
    half_dim = values.shape[-1] // 2
    inv_freq = 1.0 / rope_base ** jnp.linspace(0.0, 1.0, half_dim, dtype=jnp.float32)
    angles = positions.astype(jnp.float32)[:, None] * inv_freq[None, :]
    cosine = jnp.cos(angles)[:, None, :]
    sine = jnp.sin(angles)[:, None, :]
    first_half = values[..., :half_dim]
    second_half = values[..., half_dim:]
    return jnp.concatenate(
        [first_half * cosine - second_half * sine, first_half * sine + second_half * cosine],
        axis=-1,
    )


def trailing_sums(extended, length):
    begin = extended.shape[0] - length
    running = extended[begin:]
    results = []
    for behind in range(1, 16):
        running = running + extended[begin - behind : begin - behind + length]
        if behind + 1 in window_list:
            results.append(running)
    return results


def reshape_blocks(array):
    return array.reshape((array.shape[0] // BLOCK, BLOCK) + array.shape[1:])


def block_retention(queries, keys_in, values_in, decay_rate, initial):
    length, head_count, head_dim = queries.shape
    within = jnp.arange(BLOCK, dtype=jnp.float32)
    distance = within[:, None] - within[None, :]
    decay_mask = jnp.where(
        distance[None] >= 0,
        jnp.exp(-jnp.maximum(distance, 0.0)[None] * decay_rate[:, None, None]),
        0.0,
    )
    query_decay_factor = jnp.exp(-(within + 1.0)[:, None] * decay_rate[None, :])
    key_decay_factor = jnp.exp(-(BLOCK - 1.0 - within)[:, None] * decay_rate[None, :])
    block_decay_factor = jnp.exp(-BLOCK * decay_rate)

    def advance(state_carry, inputs):
        block_queries, block_keys, block_values = inputs
        scores = (
            jnp.einsum("ihk,jhk->hij", block_queries, block_keys, precision=highest_precision)
            * decay_mask
        )
        inside = jnp.einsum("hij,jhv->ihv", scores, block_values, precision=highest_precision)
        across_blocks = jnp.einsum(
            "bzy,zyx->bzx",
            block_queries * query_decay_factor[:, :, None],
            state_carry,
            precision=highest_precision,
        )
        state_carry = state_carry * block_decay_factor[:, None, None] + jnp.einsum(
            "flm,fld->lmd",
            block_keys * key_decay_factor[:, :, None],
            block_values,
            precision=highest_precision,
        )
        return (state_carry, inside + across_blocks)

    final_state, outputs = lax.scan(
        advance,
        initial,
        (reshape_blocks(queries), reshape_blocks(keys_in), reshape_blocks(values_in)),
    )
    return (outputs.reshape(length, head_count, values_in.shape[-1]), final_state)


def combine_states(earlier, latter):
    return (earlier[0] * latter[0], latter[0][:, None, None] * earlier[1] + latter[1])


def on_device(
    tokens,
    norm_gain,
    pool_proj,
    query_proj,
    key_proj,
    value_proj,
    pool_map,
    pool_scale,
    decay_rate,
    start_state,
    pool_back,
    retention_back,
):
    sequence = tokens[0]
    length = sequence.shape[0]
    tp_index = lax.axis_index("tp")
    sp_index = lax.axis_index("sp")
    tp_count = lax.axis_size("tp")
    floats = sequence.astype(jnp.float32)
    normed = (
        floats * lax.rsqrt(jnp.mean(floats * floats, axis=-1, keepdims=True) + eps) * norm_gain
    ).astype(jnp.bfloat16)
    group_normed = lax.all_gather(normed, "fs", axis=0, tiled=True)
    quarters = (
        lax.all_to_all(pool_proj, "fs", split_axis=1, concat_axis=0, tiled=True),
        lax.all_to_all(query_proj, "fs", split_axis=1, concat_axis=0, tiled=True),
        lax.all_to_all(key_proj, "fs", split_axis=1, concat_axis=0, tiled=True),
        lax.all_to_all(value_proj, "fs", split_axis=1, concat_axis=0, tiled=True),
    )
    pieces = (
        lax.all_gather(quarters[0], "sp", axis=0, tiled=True),
        lax.all_gather(quarters[1], "sp", axis=0, tiled=True),
        lax.all_gather(quarters[2], "sp", axis=0, tiled=True),
        lax.all_gather(quarters[3], "sp", axis=0, tiled=True),
    )
    partial_cols = tuple(
        (jnp.dot(group_normed, piece_w, preferred_element_type=jnp.float32) for piece_w in pieces)
    )
    rounded = tuple((result.astype(jnp.bfloat16) for result in partial_cols))
    pool_in, query_bf, key_bf, value_bf = jax.tree.map(
        lambda part, own: part.astype(own.dtype),
        lax.all_to_all(shortened(rounded), "fs", split_axis=0, concat_axis=1, tiled=True),
        rounded,
    )
    positions = jnp.arange(length, dtype=jnp.int32) + sp_index * length
    before = shifted(pool_in[length - HALO :], "sp", 1)
    extended = jnp.concatenate([before, pool_in], axis=0).astype(jnp.float32)
    stacked = jnp.stack(trailing_sums(extended, length))
    local_groups = GROUPS // tp_count
    channels = pool_in.shape[1]
    group_dim = channels // local_groups
    group_maps = lax.dynamic_slice_in_dim(pool_map, tp_index * local_groups, local_groups, 0)
    scales = lax.dynamic_slice_in_dim(pool_scale, tp_index * channels, channels, 0)
    windows = jnp.array(window_list, dtype=jnp.int32)
    pieces = []
    for group_idx in range(local_groups):
        chosen_group = tp_index * local_groups + group_idx
        lower = group_idx * group_dim
        chosen = lax.dynamic_index_in_dim(stacked, chosen_group, 0, keepdims=False)[
            :, lower : lower + group_dim
        ]
        counts = jnp.minimum(windows[chosen_group], positions + 1).astype(jnp.float32)
        inputs = extended[HALO:, lower : lower + group_dim]
        differ = (chosen / counts[:, None] - inputs).astype(jnp.bfloat16)
        pieces.append(jnp.dot(differ, group_maps[group_idx], preferred_element_type=jnp.float32))
    pool_out = (jnp.concatenate(pieces, axis=1) * scales).astype(jnp.bfloat16)
    head_count = decay_rate.shape[0]
    head_dim = query_bf.shape[1] // head_count
    queries = rotate(query_bf.astype(jnp.float32).reshape(length, head_count, head_dim), positions)
    keys_in = rotate(
        key_bf.astype(jnp.float32).reshape(length, head_count, head_dim), positions
    ) * head_dim ** (-0.5)
    values_in = value_bf.astype(jnp.float32).reshape(length, head_count, head_dim)
    zeros_state = jnp.zeros((head_count, head_dim, head_dim), jnp.float32)
    local_output, local_state = block_retention(
        queries, keys_in, values_in, decay_rate, zeros_state
    )
    span_decay = jnp.exp(-decay_rate * length)
    whole_start = lax.all_gather(start_state, "sp", axis=2, tiled=True)[0]
    span_factor, carried_over = carried_in(
        (span_decay, local_state), "sp", combine_states, (jnp.ones_like(span_decay), zeros_state)
    )
    offset_float = (sp_index * length).astype(jnp.float32)
    carried_over = carried_over + jnp.exp(-decay_rate * offset_float)[:, None, None] * whole_start
    steps_in = jnp.arange(length, dtype=jnp.float32) + 1.0
    query_rows_scaled = queries * jnp.exp(-steps_in[:, None] * decay_rate[None, :])[:, :, None]
    retained_output = local_output + jnp.einsum(
        "lpi,pib->lpb", query_rows_scaled, carried_over, precision=highest_precision
    )
    retained_output = retained_output * lax.rsqrt(
        jnp.mean(retained_output * retained_output, axis=-1, keepdims=True) + eps
    )
    ret_out = retained_output.reshape(length, head_count * head_dim).astype(jnp.bfloat16)
    pool_cols, retention_cols = (
        lax.all_gather(pool_back, ("sp", "fs"), axis=1, tiled=True),
        lax.all_gather(retention_back, ("sp", "fs"), axis=1, tiled=True),
    )
    weight_local = jnp.concatenate([pool_cols, retention_cols], axis=0)
    joined = jnp.concatenate([pool_out, ret_out], axis=1)
    mixed = lax.psum_scatter(
        jnp.dot(joined, weight_local, preferred_element_type=jnp.float32).astype(jnp.bfloat16),
        "tp",
        scatter_dimension=0,
        tiled=True,
    )
    return mixed[None]


MESH = pl.DeviceIdType.MESH


def where_am_i():
    sp, fs, tp = (lax.axis_index(name) for name in ("sp", "fs", "tp"))
    return sp, fs, tp, fs // 2, fs % 2


def remote(src, dst, send, recv, target):
    return pltpu.make_async_remote_copy(
        src_ref=src, dst_ref=dst, send_sem=send, recv_sem=recv, device_id=target, device_id_type=MESH
    )


def greet(others):
    barrier = pltpu.get_barrier_semaphore()
    for other in others:
        pl.semaphore_signal(barrier, inc=1, device_id=other, device_id_type=MESH)
    pl.semaphore_wait(barrier, len(others))


def cols(index, size):
    return pl.ds(pl.multiple_of(index * size, size), size)


def project_kernel(
    tok, gain, wp, wq, wk, wv, state, pb, rb,
    joined, start, backs,
    xn, xg, wg, part, got,
    w_send, w_recv, w_local, x_send, x_recv, x_local, f_send, f_recv,
    s_send, s_recv, b_send, b_recv, b_local, p_send, p_recv, j_send, j_recv,
):
    sp, fs, tp, y, x = where_am_i()
    nsp, nfs = 4, 4
    span, width = tok.shape
    half = span // 2
    feats = width // nsp
    rows, group = wg.shape[2], wg.shape[3]
    mats = (wp, wq, wk, wv)
    partner = (sp, fs, 1 - tp)
    waits = []
    greet(
        [
            (lax.rem(sp + dz, nsp), 2 * lax.rem(y + dy, 2) + x, lax.rem(tp + dt, 2))
            for dz in range(nsp) for dy in range(2) for dt in range(2) if dz or dy or dt
        ]
        + [(sp, 2 * lax.rem(y + dy, 2) + 1 - x, tp) for dy in range(2)]
    )

    def send_mat(m):
        for d in (3, 1, 2):
            to = lax.rem(fs + d, nfs)
            c = remote(
                mats[m].at[:, cols(to // 2, group)], wg.at[m, fs], w_send.at[d - 1, m],
                w_recv.at[m, fs], (sp, to, tp),
            )
            c.start()
            waits.append(c)
        c = pltpu.make_async_copy(mats[m].at[:, cols(y, group)], wg.at[m, fs], w_local.at[m])
        c.start()
        return c

    own_w = [send_mat(0)]

    floats = tok[...].astype(jnp.float32)
    xn[...] = (
        floats * lax.rsqrt(jnp.mean(floats * floats, axis=-1, keepdims=True) + eps) * gain[...]
    ).astype(jnp.bfloat16)

    mine = pl.ds(pl.multiple_of(tp * half, half), half)

    def slot_of(from_y, from_sp):
        return xg.at[from_y, pl.ds(pl.multiple_of(from_sp * span + tp * half, half), half)]

    peer = (sp, 2 * (1 - y) + x, tp)
    for dz in (2, 1, 3, 0):
        to_sp = lax.rem(sp + dz, nsp)
        c = remote(
            xn.at[mine, cols(to_sp, feats)], slot_of(y, sp), x_send.at[dz], x_recv.at[y, sp],
            (to_sp, fs, tp) if dz else peer,
        )
        c.start()
        waits.append(c)
    own_x = pltpu.make_async_copy(
        xn.at[:, cols(sp, feats)], xg.at[y, pl.ds(pl.multiple_of(sp * span, span), span)], x_local
    )
    own_x.start()
    own_w.append(send_mat(1))
    forwards = []

    def arrived(from_y, from_sp, order):
        slot = slot_of(from_y, from_sp)
        remote(slot, slot, x_send.at[0], x_recv.at[from_y, from_sp], partner).wait_recv()
        c = remote(slot, slot, f_send.at[order], f_recv.at[order], partner)
        c.start()
        forwards.append(c)
        return slot

    for dz in (1, 3, 2):
        fr_sp = lax.rem(sp + nsp - dz, nsp)
        slot = arrived(y, fr_sp, dz - 1)
        c = remote(slot, slot, x_send.at[nsp + dz - 1], x_recv.at[y, fr_sp], peer)
        c.start()
        waits.append(c)
    for m in range(2, 4):
        own_w.append(send_mat(m))
    for j in range(2):
        for h in range(2):
            to_sp, to_fs = 2 * y + tp, 2 * j + x
            rs = state.shape[1]
            dst = start.at[pl.ds(pl.multiple_of(sp * rs, rs), rs)]
            same = (to_sp == sp) & (to_fs == fs) & (tp == h)

            @pl.when(same)
            def _():
                pltpu.make_async_copy(state.at[j], dst, s_recv.at[sp]).start()

            @pl.when(jnp.logical_not(same))
            def _():
                remote(state.at[j], dst, s_send.at[2 * j + h], s_recv.at[sp], (to_sp, to_fs, h)).start()

    own_b = []
    for b, back in enumerate((pb, rb)):
        c = pltpu.make_async_copy(back, backs.at[fs, b], b_local.at[b])
        c.start()
        own_b.append(c)
        for d in (3, 1, 2):
            to = lax.rem(fs + d, nfs)
            c = remote(back, backs.at[fs, b], b_send.at[d - 1, b], b_recv.at[fs, b], (sp, to, tp))
            c.start()
            waits.append(c)

    for dz in (0, 1, 3, 2):
        arrived(1 - y, lax.rem(sp + nsp - dz, nsp), 3 + dz)
    own_x.wait()
    for c in forwards:
        c.wait()

    tall = 2 * span
    for m in range(4):
        own_w[m].wait()
        for d in range(1, nfs):
            fr = lax.rem(fs + nfs - d, nfs)
            remote(
                mats[m].at[:, cols(y, group)], wg.at[m, fr], w_send.at[d - 1, m], w_recv.at[m, fr], partner
            ).wait_recv()
        for s in range(2):
            acc = jnp.zeros((2 * tall, group), jnp.float32)
            for f in range(nfs):
                acc += jnp.dot(
                    xg[s, :, f * rows : (f + 1) * rows], wg[m, f], preferred_element_type=jnp.float32
                )
            part[m, s] = acc.astype(jnp.bfloat16)
            for h in range(2):
                same = (2 * s + tp == sp) & (tp == h)
                src = part.at[m, s, h * tall : (h + 1) * tall]

                @pl.when(same)
                def _():
                    pltpu.make_async_copy(src, got.at[m, sp], p_recv.at[m, sp]).start()

                @pl.when(jnp.logical_not(same))
                def _():
                    remote(
                        src, got.at[m, sp], p_send.at[m, 2 * s + h], p_recv.at[m, sp], (2 * s + tp, fs, h)
                    ).start()

    here = pl.ds(pl.multiple_of(tp * tall, tall), tall)
    there = pl.ds(pl.multiple_of((1 - tp) * tall, tall), tall)
    lasts = []
    for m in range(4):
        for k in range(nsp):
            remote(got.at[m, k], got.at[m, k], p_send.at[0, 0], p_recv.at[m, k], partner).wait_recv()
        total = got[m, 0].astype(jnp.float32)
        for k in range(1, nsp):
            total += got[m, k].astype(jnp.float32)
        joined[m, here] = total.astype(jnp.bfloat16)
        c = remote(joined.at[m, here], joined.at[m, here], j_send.at[m], j_recv.at[m], partner)
        c.start()
        lasts.append(c)
    for m in range(4):
        lasts[m].wait_send()
        remote(joined.at[m, there], joined.at[m, there], j_send.at[m], j_recv.at[m], partner).wait_recv()

    for j in range(2):
        for h in range(2):
            to_sp, to_fs = 2 * y + tp, 2 * j + x
            same = (to_sp == sp) & (to_fs == fs) & (tp == h)

            @pl.when(jnp.logical_not(same))
            def _():
                remote(state.at[j], start.at[pl.ds(0, state.shape[1])], s_send.at[2 * j + h], s_recv.at[0], partner).wait_send()

            same_p = (2 * j + tp == sp) & (tp == h)

            @pl.when(jnp.logical_not(same_p))
            def _():
                for m in range(4):
                    remote(got.at[m, 0], got.at[m, 0], p_send.at[m, 2 * j + h], p_recv.at[m, 0], partner).wait_send()

    for k in range(nsp):
        rs = state.shape[1]
        slot = start.at[k * rs : (k + 1) * rs]
        remote(slot, slot, s_send.at[0], s_recv.at[k], partner).wait_recv()
    for b, back in enumerate((pb, rb)):
        own_b[b].wait()
        for d in range(1, nfs):
            fr = lax.rem(fs + nfs - d, nfs)
            remote(back, backs.at[fr, b], b_send.at[d - 1, b], b_recv.at[fr, b], partner).wait_recv()
    for c in waits:
        c.wait_send()


def output_kernel(
    yh, backs, out,
    yg, stage, accs, give, take, done,
    y_send, y_recv, t_send, t_recv, g_send, g_recv, o_send, o_recv,
):
    sp, fs, tp, y, x = where_am_i()
    nsp, nfs = 4, 4
    half, wide = yh.shape
    group = wide // 2
    block = backs.shape[3]
    few = out.shape[0]
    across = nfs * block
    partner = (sp, fs, 1 - tp)
    s, p = sp // 2, sp % 2
    peer = (sp, 2 * (1 - y) + x, tp)
    greet(
        [
            (lax.rem(sp + dz, nsp), fs, lax.rem(tp + dt, 2))
            for dz in range(nsp) for dt in range(2) if dz or dt
        ]
        + [peer]
    )
    few2 = half // 2
    for c in range(2):
        part = yh.at[c * few2 : (c + 1) * few2]
        for dz in (2, 1, 3, 0):
            k = lax.rem(sp + dz, nsp)
            for staged, dst, sem in (
                (False, yg.at[y, tp, c], y_recv.at[y, tp, c]), (True, stage.at[tp, c], t_recv.at[tp, c])
            ):
                kind = (s != y) if staged else (s == y)
                if dz:

                    @pl.when(kind)
                    def _():
                        remote(part, dst, y_send.at[dz, c], sem, (k, fs, p)).start()
                else:

                    @pl.when(kind & (p == tp))
                    def _():
                        pltpu.make_async_copy(part, dst, sem).start()

                    @pl.when(kind & (p != tp))
                    def _():
                        remote(part, dst, y_send.at[dz, c], sem, partner).start()

    passed = []

    def forward(c):
        for h in range(2):
            slot = stage.at[h, c]
            remote(slot, slot, y_send.at[0, 0], t_recv.at[h, c], partner).wait_recv()
            move = remote(slot, yg.at[y, h, c], t_send.at[h, c], y_recv.at[y, h, c], peer)
            move.start()
            passed.append(move)

    def multiply(c):
        gives = []
        for h in range(2):
            for q in range(2):
                slot = yg.at[q, h, c]
                remote(slot, slot, y_send.at[0, 0], y_recv.at[q, h, c], partner).wait_recv()
            k = 2 * h + c
            for f in range(nfs):
                acc = jnp.zeros((few2, block), jnp.float32)
                for q in range(2):
                    for b in range(2):
                        acc += jnp.dot(
                            yg[q, h, c, :, b * group : (b + 1) * group],
                            backs[f, b, q * group : (q + 1) * group, :],
                            preferred_element_type=jnp.float32,
                        )
                accs[k, :, f * block : (f + 1) * block] = acc
            give[k] = accs[k, pl.ds(pl.multiple_of((1 - tp) * few, few), few), :].astype(jnp.bfloat16)
            move = remote(give.at[k], take.at[k], g_send.at[k], g_recv.at[k], partner)
            move.start()
            gives.append(move)
        return gives

    def finish(c, gives):
        for h in range(2):
            k = 2 * h + c
            gives[h].wait()
            own = accs[k, pl.ds(pl.multiple_of(tp * few, few), few), :]
            done[k] = (own + take[k].astype(jnp.float32)).astype(jnp.bfloat16)
            dst = out.at[:, cols(sp, across)]

            @pl.when(sp == k)
            def _():
                pltpu.make_async_copy(done.at[k], dst, o_recv.at[sp]).start()

            @pl.when(sp != k)
            def _():
                remote(done.at[k], dst, o_send.at[k], o_recv.at[sp], (k, fs, tp)).start()

    forward(0)
    first = multiply(0)
    finish(0, first)
    forward(1)
    second = multiply(1)
    finish(1, second)

    for k in range(nsp):
        view = out.at[:, k * across : (k + 1) * across]
        remote(done.at[k], view, o_send.at[k], o_recv.at[k], partner).wait_recv()

        @pl.when(sp != k)
        def _():
            remote(done.at[k], view, o_send.at[k], o_recv.at[k], partner).wait_send()

    for c in range(2):
        slot = yg.at[0, 0, c]
        for dz in range(1, nsp):
            remote(slot, slot, y_send.at[dz, c], y_recv.at[0, 0, c], partner).wait_send()

        @pl.when(p != tp)
        def _():
            remote(slot, slot, y_send.at[0, c], y_recv.at[0, 0, c], partner).wait_send()

    for move in passed:
        move.wait_send()


def turned(values, cosine, sine):
    half_dim = values.shape[-1] // 2
    a, b = values[:, :half_dim], values[:, half_dim:]
    return jnp.concatenate([a * cosine - b * sine, a * sine + b * cosine], axis=-1)


def angles_of(positions, half_dim):
    inv_freq = 1.0 / rope_base ** jnp.linspace(0.0, 1.0, half_dim, dtype=jnp.float32)
    angles = positions.astype(jnp.float32)[:, None] * inv_freq[None, :]
    return jnp.cos(angles), jnp.sin(angles)


def paired(
    tokens, norm_gain, pool_proj, query_proj, key_proj, value_proj, pool_map, pool_scale,
    decay_rate, start_state, pool_back, retention_back,
):
    bf, f32 = jnp.bfloat16, jnp.float32
    sp, fs, tp, y, x = where_am_i()
    nsp = lax.axis_size("sp")
    tok = tokens[0]
    span, width = tok.shape
    rows, two = pool_proj.shape
    group = two // 2
    length = nsp * span
    half = length // 2
    vm, hbm = pl.BlockSpec(memory_space=pltpu.VMEM), pl.BlockSpec(memory_space=pl.ANY)
    dma = pltpu.SemaphoreType.DMA
    rs = start_state.shape[2]
    joined, start, backs = pl.pallas_call(
        project_kernel,
        out_shape=(
            jax.ShapeDtypeStruct((4, length, group), bf),
            jax.ShapeDtypeStruct((nsp * rs, group), bf),
            jax.ShapeDtypeStruct((4, 2) + pool_back.shape, bf),
        ),
        in_specs=[vm, vm, hbm, hbm, hbm, hbm, hbm, hbm, hbm],
        out_specs=(vm, vm, vm),
        scratch_shapes=[
            pltpu.VMEM((span, width), bf),
            pltpu.VMEM((2, nsp * span, width // nsp), bf),
            pltpu.VMEM((4, 4, rows, group), bf),
            pltpu.VMEM((4, 2, length, group), bf),
            pltpu.VMEM((4, nsp, half, group), bf),
            dma((3, 4)), dma((4, 4)), dma((4,)), dma((7,)), dma((2, nsp)), dma,
            dma((7,)), dma((7,)), dma((4,)), dma((nsp,)), dma((3, 2)), dma((4, 2)), dma((2,)),
            dma((4, 4)), dma((4, nsp)), dma((4,)), dma((4,)),
        ],
        compiler_params=pltpu.CompilerParams(collective_id=0, has_side_effects=True, vmem_limit_bytes=60 * 2**20),
        name="project",
    )(
        tok, norm_gain[None, :], pool_proj, query_proj, key_proj, value_proj,
        start_state[0].astype(bf), pool_back, retention_back,
    )
    mine = lax.dynamic_slice_in_dim(joined[1], tp * half, half, 0)
    head = 2 * (sp % 2) + y
    local = lax.dynamic_index_in_dim(decay_rate, y, 0, keepdims=False)
    other = lax.ppermute(decay_rate, "tp", [(0, 1), (1, 0)])
    rate = jnp.where(sp % 2 == tp, local, lax.dynamic_index_in_dim(other, y, 0, keepdims=False))
    every = jnp.arange(length, dtype=jnp.int32)
    position = tp * half + jnp.arange(half, dtype=jnp.int32)

    pool_all = jnp.concatenate([jnp.zeros((HALO, group), f32), joined[0].astype(f32)], axis=0)
    extended = lax.dynamic_slice_in_dim(pool_all, tp * half, half + HALO, 0)
    sums = trailing_sums(extended, half)
    windows = jnp.array(window_list, dtype=jnp.int32)
    chosen = sums[0]
    for i in range(1, GROUPS):
        chosen = jnp.where(head == i, sums[i], chosen)
    counts = jnp.minimum(windows[head], position + 1).astype(f32)
    differ = (chosen / counts[:, None] - extended[HALO:]).astype(bf)
    this_map = lax.dynamic_index_in_dim(pool_map, head, 0, keepdims=False)
    scale = lax.dynamic_slice_in_dim(pool_scale, head * group, group, 0)
    pool_out = (jnp.dot(differ, this_map, preferred_element_type=f32) * scale).astype(bf)

    cosine, sine = angles_of(every, group // 2)
    my_cos = lax.dynamic_slice_in_dim(cosine, tp * half, half, 0)
    my_sin = lax.dynamic_slice_in_dim(sine, tp * half, half, 0)
    rq = turned(mine.astype(f32), my_cos, my_sin)
    rk = turned(joined[2].astype(f32), cosine, sine) * group ** (-0.5)
    value = joined[3].astype(f32)
    gap = (position[:, None] - every[None, :]).astype(f32)
    mask = jnp.where(gap >= 0, jnp.exp(-jnp.maximum(gap, 0.0) * rate), 0.0)
    high = lax.Precision.HIGHEST
    scores = jnp.dot(rq, rk.T, precision=high) * mask
    fade = jnp.exp(-(position.astype(f32) + 1.0) * rate)
    ret = jnp.dot(scores, value, precision=high) + jnp.dot(
        rq * fade[:, None], start.astype(f32), precision=high
    )
    ret = ret * lax.rsqrt(jnp.mean(ret * ret, axis=-1, keepdims=True) + eps)
    yh = jnp.concatenate([pool_out, ret.astype(bf)], axis=1)

    few = span // 2
    return pl.pallas_call(
        output_kernel,
        out_shape=jax.ShapeDtypeStruct((few, width), bf),
        in_specs=[vm, vm],
        out_specs=vm,
        scratch_shapes=[
            pltpu.VMEM((2, 2, 2, span, 2 * group), bf),
            pltpu.VMEM((2, 2, span, 2 * group), bf),
            pltpu.VMEM((nsp, span, 4 * pool_back.shape[1]), f32),
            pltpu.VMEM((nsp, few, 4 * pool_back.shape[1]), bf),
            pltpu.VMEM((nsp, few, 4 * pool_back.shape[1]), bf),
            pltpu.VMEM((nsp, few, 4 * pool_back.shape[1]), bf),
            dma((nsp, 2)), dma((2, 2, 2)), dma((2, 2)), dma((2, 2)), dma((nsp,)), dma((nsp,)), dma((nsp,)), dma((nsp,)),
        ],
        compiler_params=pltpu.CompilerParams(collective_id=1, has_side_effects=True, vmem_limit_bytes=60 * 2**20),
        name="output",
    )(yh, backs)[None]


def solution(mesh):
    sizes = mesh.shape
    small = sizes["sp"] == 4 and sizes["fs"] == 4 and sizes["tp"] == 2
    placed = (
        P("fs", "sp", None),
        P(),
        P(("sp", "fs"), "tp"),
        P(("sp", "fs"), "tp"),
        P(("sp", "fs"), "tp"),
        P(("sp", "fs"), "tp"),
        P(),
        P(),
        P("tp"),
        P("fs", "tp", "sp", None),
        P("tp", ("sp", "fs")),
        P("tp", ("sp", "fs")),
    )
    return jax.shard_map(
        paired if small else on_device,
        mesh=mesh,
        in_specs=placed,
        out_specs=P("fs", ("sp", "tp"), None),
        check_vma=False,
    )
```

```python
import functools

from jax.experimental import pallas as pl
from jax.experimental.pallas import tpu as pltpu

import jax
import jax.numpy as jnp
from jax import lax
from jax.sharding import PartitionSpec as P

GROUPS = 4
BLOCK = 128
HALO = 16


eps = 1e-06
rope_base = 10000.0
highest_precision = lax.Precision.HIGHEST
window_list = (2, 4, 8, 16)


def shortened(x):
    return jax.tree.map(lambda a: a.astype(jnp.bfloat16) if a.dtype == jnp.float32 else a, x)


def shifted(x, axis, by):
    devices = lax.axis_size(axis)
    pairs = [(i, i + by) for i in range(devices) if 0 <= i + by < devices]
    return lax.ppermute(x, axis, pairs)


def carried_in(value, axis, join, neutral):
    count, mine = (lax.axis_size(axis), lax.axis_index(axis))
    pieces = jax.tree.map(lambda part: lax.all_gather(part, axis), value)
    running = jax.tree.map(
        lambda part, zero: jnp.full_like(part, 0) + jnp.asarray(zero, part.dtype), value, neutral
    )

    def turn(position, running):
        longer = join(running, jax.tree.map(lambda part: part[position], pieces))
        return jax.tree.map(lambda new, old: jnp.where(position < mine, new, old), longer, running)

    return lax.fori_loop(0, count - 1, turn, running)


def rotate(values, positions):
    half_dim = values.shape[-1] // 2
    inv_freq = 1.0 / rope_base ** jnp.linspace(0.0, 1.0, half_dim, dtype=jnp.float32)
    angles = positions.astype(jnp.float32)[:, None] * inv_freq[None, :]
    cosine = jnp.cos(angles)[:, None, :]
    sine = jnp.sin(angles)[:, None, :]
    first_half = values[..., :half_dim]
    second_half = values[..., half_dim:]
    return jnp.concatenate(
        [first_half * cosine - second_half * sine, first_half * sine + second_half * cosine],
        axis=-1,
    )


def trailing_sums(extended, length):
    begin = extended.shape[0] - length
    running = extended[begin:]
    results = []
    for behind in range(1, 16):
        running = running + extended[begin - behind : begin - behind + length]
        if behind + 1 in window_list:
            results.append(running)
    return results


def reshape_blocks(array):
    return array.reshape((array.shape[0] // BLOCK, BLOCK) + array.shape[1:])


def block_retention(queries, keys_in, values_in, decay_rate, initial):
    length, head_count, head_dim = queries.shape
    within = jnp.arange(BLOCK, dtype=jnp.float32)
    distance = within[:, None] - within[None, :]
    decay_mask = jnp.where(
        distance[None] >= 0,
        jnp.exp(-jnp.maximum(distance, 0.0)[None] * decay_rate[:, None, None]),
        0.0,
    )
    query_decay_factor = jnp.exp(-(within + 1.0)[:, None] * decay_rate[None, :])
    key_decay_factor = jnp.exp(-(BLOCK - 1.0 - within)[:, None] * decay_rate[None, :])
    block_decay_factor = jnp.exp(-BLOCK * decay_rate)

    def advance(state_carry, inputs):
        block_queries, block_keys, block_values = inputs
        scores = (
            jnp.einsum("ihk,jhk->hij", block_queries, block_keys, precision=highest_precision)
            * decay_mask
        )
        inside = jnp.einsum("hij,jhv->ihv", scores, block_values, precision=highest_precision)
        across_blocks = jnp.einsum(
            "bzy,zyx->bzx",
            block_queries * query_decay_factor[:, :, None],
            state_carry,
            precision=highest_precision,
        )
        state_carry = state_carry * block_decay_factor[:, None, None] + jnp.einsum(
            "flm,fld->lmd",
            block_keys * key_decay_factor[:, :, None],
            block_values,
            precision=highest_precision,
        )
        return (state_carry, inside + across_blocks)

    final_state, outputs = lax.scan(
        advance,
        initial,
        (reshape_blocks(queries), reshape_blocks(keys_in), reshape_blocks(values_in)),
    )
    return (outputs.reshape(length, head_count, values_in.shape[-1]), final_state)


def combine_states(earlier, latter):
    return (earlier[0] * latter[0], latter[0][:, None, None] * earlier[1] + latter[1])


def on_device(
    tokens,
    norm_gain,
    pool_proj,
    query_proj,
    key_proj,
    value_proj,
    pool_map,
    pool_scale,
    decay_rate,
    start_state,
    pool_back,
    retention_back,
):
    sequence = tokens[0]
    length = sequence.shape[0]
    tp_index = lax.axis_index("tp")
    sp_index = lax.axis_index("sp")
    tp_count = lax.axis_size("tp")
    floats = sequence.astype(jnp.float32)
    normed = (
        floats * lax.rsqrt(jnp.mean(floats * floats, axis=-1, keepdims=True) + eps) * norm_gain
    ).astype(jnp.bfloat16)
    group_normed = lax.all_gather(normed, "fs", axis=0, tiled=True)
    quarters = (
        lax.all_to_all(pool_proj, "fs", split_axis=1, concat_axis=0, tiled=True),
        lax.all_to_all(query_proj, "fs", split_axis=1, concat_axis=0, tiled=True),
        lax.all_to_all(key_proj, "fs", split_axis=1, concat_axis=0, tiled=True),
        lax.all_to_all(value_proj, "fs", split_axis=1, concat_axis=0, tiled=True),
    )
    pieces = (
        lax.all_gather(quarters[0], "sp", axis=0, tiled=True),
        lax.all_gather(quarters[1], "sp", axis=0, tiled=True),
        lax.all_gather(quarters[2], "sp", axis=0, tiled=True),
        lax.all_gather(quarters[3], "sp", axis=0, tiled=True),
    )
    partial_cols = tuple(
        (jnp.dot(group_normed, piece_w, preferred_element_type=jnp.float32) for piece_w in pieces)
    )
    rounded = tuple((result.astype(jnp.bfloat16) for result in partial_cols))
    pool_in, query_bf, key_bf, value_bf = jax.tree.map(
        lambda part, own: part.astype(own.dtype),
        lax.all_to_all(shortened(rounded), "fs", split_axis=0, concat_axis=1, tiled=True),
        rounded,
    )
    positions = jnp.arange(length, dtype=jnp.int32) + sp_index * length
    before = shifted(pool_in[length - HALO :], "sp", 1)
    extended = jnp.concatenate([before, pool_in], axis=0).astype(jnp.float32)
    stacked = jnp.stack(trailing_sums(extended, length))
    local_groups = GROUPS // tp_count
    channels = pool_in.shape[1]
    group_dim = channels // local_groups
    group_maps = lax.dynamic_slice_in_dim(pool_map, tp_index * local_groups, local_groups, 0)
    scales = lax.dynamic_slice_in_dim(pool_scale, tp_index * channels, channels, 0)
    windows = jnp.array(window_list, dtype=jnp.int32)
    pieces = []
    for group_idx in range(local_groups):
        chosen_group = tp_index * local_groups + group_idx
        lower = group_idx * group_dim
        chosen = lax.dynamic_index_in_dim(stacked, chosen_group, 0, keepdims=False)[
            :, lower : lower + group_dim
        ]
        counts = jnp.minimum(windows[chosen_group], positions + 1).astype(jnp.float32)
        inputs = extended[HALO:, lower : lower + group_dim]
        differ = (chosen / counts[:, None] - inputs).astype(jnp.bfloat16)
        pieces.append(jnp.dot(differ, group_maps[group_idx], preferred_element_type=jnp.float32))
    pool_out = (jnp.concatenate(pieces, axis=1) * scales).astype(jnp.bfloat16)
    head_count = decay_rate.shape[0]
    head_dim = query_bf.shape[1] // head_count
    queries = rotate(query_bf.astype(jnp.float32).reshape(length, head_count, head_dim), positions)
    keys_in = rotate(
        key_bf.astype(jnp.float32).reshape(length, head_count, head_dim), positions
    ) * head_dim ** (-0.5)
    values_in = value_bf.astype(jnp.float32).reshape(length, head_count, head_dim)
    zeros_state = jnp.zeros((head_count, head_dim, head_dim), jnp.float32)
    local_output, local_state = block_retention(
        queries, keys_in, values_in, decay_rate, zeros_state
    )
    span_decay = jnp.exp(-decay_rate * length)
    whole_start = lax.all_gather(start_state, "sp", axis=2, tiled=True)[0]
    span_factor, carried_over = carried_in(
        (span_decay, local_state), "sp", combine_states, (jnp.ones_like(span_decay), zeros_state)
    )
    offset_float = (sp_index * length).astype(jnp.float32)
    carried_over = carried_over + jnp.exp(-decay_rate * offset_float)[:, None, None] * whole_start
    steps_in = jnp.arange(length, dtype=jnp.float32) + 1.0
    query_rows_scaled = queries * jnp.exp(-steps_in[:, None] * decay_rate[None, :])[:, :, None]
    retained_output = local_output + jnp.einsum(
        "lpi,pib->lpb", query_rows_scaled, carried_over, precision=highest_precision
    )
    retained_output = retained_output * lax.rsqrt(
        jnp.mean(retained_output * retained_output, axis=-1, keepdims=True) + eps
    )
    ret_out = retained_output.reshape(length, head_count * head_dim).astype(jnp.bfloat16)
    pool_cols, retention_cols = (
        lax.all_gather(pool_back, ("sp", "fs"), axis=1, tiled=True),
        lax.all_gather(retention_back, ("sp", "fs"), axis=1, tiled=True),
    )
    weight_local = jnp.concatenate([pool_cols, retention_cols], axis=0)
    joined = jnp.concatenate([pool_out, ret_out], axis=1)
    mixed = lax.psum_scatter(
        jnp.dot(joined, weight_local, preferred_element_type=jnp.float32).astype(jnp.bfloat16),
        "tp",
        scatter_dimension=0,
        tiled=True,
    )
    return mixed[None]


MESH = pl.DeviceIdType.MESH


def where_am_i():
    sp, fs, tp = (lax.axis_index(name) for name in ("sp", "fs", "tp"))
    return sp, fs, tp, fs // 2, fs % 2


def remote(src, dst, send, recv, target):
    return pltpu.make_async_remote_copy(
        src_ref=src, dst_ref=dst, send_sem=send, recv_sem=recv, device_id=target, device_id_type=MESH
    )


def greet(others):
    barrier = pltpu.get_barrier_semaphore()
    for other in others:
        pl.semaphore_signal(barrier, inc=1, device_id=other, device_id_type=MESH)
    pl.semaphore_wait(barrier, len(others))


def cols(index, size):
    return pl.ds(pl.multiple_of(index * size, size), size)


def project_kernel(
    tok, gain, wp, wq, wk, wv, state, pb, rb,
    joined, start, backs,
    xn, xg, wg, part, got,
    w_send, w_recv, w_local, x_send, x_recv, x_local, f_send, f_recv,
    s_send, s_recv, b_send, b_recv, b_local, p_send, p_recv, j_send, j_recv,
):
    sp, fs, tp, y, x = where_am_i()
    nsp, nfs = 4, 4
    span, width = tok.shape
    half = span // 2
    feats = width // nsp
    rows, group = wg.shape[2], wg.shape[3]
    mats = (wp, wq, wk, wv)
    partner = (sp, fs, 1 - tp)
    waits = []
    greet(
        [
            (lax.rem(sp + dz, nsp), 2 * lax.rem(y + dy, 2) + x, lax.rem(tp + dt, 2))
            for dz in range(nsp) for dy in range(2) for dt in range(2) if dz or dy or dt
        ]
        + [(sp, 2 * lax.rem(y + dy, 2) + 1 - x, tp) for dy in range(2)]
    )

    def send_mat(m):
        for d in (3, 1, 2):
            to = lax.rem(fs + d, nfs)
            c = remote(
                mats[m].at[:, cols(to // 2, group)], wg.at[m, fs], w_send.at[d - 1, m],
                w_recv.at[m, fs], (sp, to, tp),
            )
            c.start()
            waits.append(c)
        c = pltpu.make_async_copy(mats[m].at[:, cols(y, group)], wg.at[m, fs], w_local.at[m])
        c.start()
        return c

    own_w = [send_mat(0)]

    floats = tok[...].astype(jnp.float32)
    xn[...] = (
        floats * lax.rsqrt(jnp.mean(floats * floats, axis=-1, keepdims=True) + eps) * gain[...]
    ).astype(jnp.bfloat16)

    mine = pl.ds(pl.multiple_of(tp * half, half), half)

    def slot_of(from_y, from_sp):
        return xg.at[from_y, pl.ds(pl.multiple_of(from_sp * span + tp * half, half), half)]

    peer = (sp, 2 * (1 - y) + x, tp)
    for dz in (2, 1, 3, 0):
        to_sp = lax.rem(sp + dz, nsp)
        c = remote(
            xn.at[mine, cols(to_sp, feats)], slot_of(y, sp), x_send.at[dz], x_recv.at[y, sp],
            (to_sp, fs, tp) if dz else peer,
        )
        c.start()
        waits.append(c)
    own_x = pltpu.make_async_copy(
        xn.at[:, cols(sp, feats)], xg.at[y, pl.ds(pl.multiple_of(sp * span, span), span)], x_local
    )
    own_x.start()
    forwards = []

    def arrived(from_y, from_sp, order):
        slot = slot_of(from_y, from_sp)
        remote(slot, slot, x_send.at[0], x_recv.at[from_y, from_sp], partner).wait_recv()
        c = remote(slot, slot, f_send.at[order], f_recv.at[order], partner)
        c.start()
        forwards.append(c)
        return slot

    for dz in (1, 3, 2):
        fr_sp = lax.rem(sp + nsp - dz, nsp)
        slot = arrived(y, fr_sp, dz - 1)
        c = remote(slot, slot, x_send.at[nsp + dz - 1], x_recv.at[y, fr_sp], peer)
        c.start()
        waits.append(c)
    for m in range(1, 4):
        own_w.append(send_mat(m))
    for j in range(2):
        for h in range(2):
            to_sp, to_fs = 2 * y + tp, 2 * j + x
            rs = state.shape[1]
            dst = start.at[pl.ds(pl.multiple_of(sp * rs, rs), rs)]
            same = (to_sp == sp) & (to_fs == fs) & (tp == h)

            @pl.when(same)
            def _():
                pltpu.make_async_copy(state.at[j], dst, s_recv.at[sp]).start()

            @pl.when(jnp.logical_not(same))
            def _():
                remote(state.at[j], dst, s_send.at[2 * j + h], s_recv.at[sp], (to_sp, to_fs, h)).start()

    own_b = []
    for b, back in enumerate((pb, rb)):
        c = pltpu.make_async_copy(back, backs.at[fs, b], b_local.at[b])
        c.start()
        own_b.append(c)
        for d in (3, 1, 2):
            to = lax.rem(fs + d, nfs)
            c = remote(back, backs.at[fs, b], b_send.at[d - 1, b], b_recv.at[fs, b], (sp, to, tp))
            c.start()
            waits.append(c)

    for dz in (0, 1, 3, 2):
        arrived(1 - y, lax.rem(sp + nsp - dz, nsp), 3 + dz)
    own_x.wait()
    for c in forwards:
        c.wait()

    tall = 2 * span
    for m in range(4):
        own_w[m].wait()
        for d in range(1, nfs):
            fr = lax.rem(fs + nfs - d, nfs)
            remote(
                mats[m].at[:, cols(y, group)], wg.at[m, fr], w_send.at[d - 1, m], w_recv.at[m, fr], partner
            ).wait_recv()
        for s in range(2):
            acc = jnp.zeros((2 * tall, group), jnp.float32)
            for f in range(nfs):
                acc += jnp.dot(
                    xg[s, :, f * rows : (f + 1) * rows], wg[m, f], preferred_element_type=jnp.float32
                )
            part[m, s] = acc.astype(jnp.bfloat16)
            for h in range(2):
                same = (2 * s + tp == sp) & (tp == h)
                src = part.at[m, s, h * tall : (h + 1) * tall]

                @pl.when(same)
                def _():
                    pltpu.make_async_copy(src, got.at[m, sp], p_recv.at[m, sp]).start()

                @pl.when(jnp.logical_not(same))
                def _():
                    remote(
                        src, got.at[m, sp], p_send.at[m, 2 * s + h], p_recv.at[m, sp], (2 * s + tp, fs, h)
                    ).start()

    here = pl.ds(pl.multiple_of(tp * tall, tall), tall)
    there = pl.ds(pl.multiple_of((1 - tp) * tall, tall), tall)
    lasts = []
    for m in range(4):
        for k in range(nsp):
            remote(got.at[m, k], got.at[m, k], p_send.at[0, 0], p_recv.at[m, k], partner).wait_recv()
        total = got[m, 0].astype(jnp.float32)
        for k in range(1, nsp):
            total += got[m, k].astype(jnp.float32)
        joined[m, here] = total.astype(jnp.bfloat16)
        c = remote(joined.at[m, here], joined.at[m, here], j_send.at[m], j_recv.at[m], partner)
        c.start()
        lasts.append(c)
    for m in range(4):
        lasts[m].wait_send()
        remote(joined.at[m, there], joined.at[m, there], j_send.at[m], j_recv.at[m], partner).wait_recv()

    for j in range(2):
        for h in range(2):
            to_sp, to_fs = 2 * y + tp, 2 * j + x
            same = (to_sp == sp) & (to_fs == fs) & (tp == h)

            @pl.when(jnp.logical_not(same))
            def _():
                remote(state.at[j], start.at[pl.ds(0, state.shape[1])], s_send.at[2 * j + h], s_recv.at[0], partner).wait_send()

            same_p = (2 * j + tp == sp) & (tp == h)

            @pl.when(jnp.logical_not(same_p))
            def _():
                for m in range(4):
                    remote(got.at[m, 0], got.at[m, 0], p_send.at[m, 2 * j + h], p_recv.at[m, 0], partner).wait_send()

    for k in range(nsp):
        rs = state.shape[1]
        slot = start.at[k * rs : (k + 1) * rs]
        remote(slot, slot, s_send.at[0], s_recv.at[k], partner).wait_recv()
    for b, back in enumerate((pb, rb)):
        own_b[b].wait()
        for d in range(1, nfs):
            fr = lax.rem(fs + nfs - d, nfs)
            remote(back, backs.at[fr, b], b_send.at[d - 1, b], b_recv.at[fr, b], partner).wait_recv()
    for c in waits:
        c.wait_send()


def output_kernel(
    yh, backs, out,
    yg, stage, accs, give, take, done,
    y_send, y_recv, t_send, t_recv, g_send, g_recv, o_send, o_recv,
):
    sp, fs, tp, y, x = where_am_i()
    nsp, nfs = 4, 4
    half, wide = yh.shape
    group = wide // 2
    block = backs.shape[3]
    few = out.shape[0]
    across = nfs * block
    partner = (sp, fs, 1 - tp)
    s, p = sp // 2, sp % 2
    peer = (sp, 2 * (1 - y) + x, tp)
    greet(
        [
            (lax.rem(sp + dz, nsp), fs, lax.rem(tp + dt, 2))
            for dz in range(nsp) for dt in range(2) if dz or dt
        ]
        + [peer]
    )
    few2 = half // 2
    for c in range(2):
        part = yh.at[c * few2 : (c + 1) * few2]
        for dz in (2, 1, 3, 0):
            k = lax.rem(sp + dz, nsp)
            for staged, dst, sem in (
                (False, yg.at[y, tp, c], y_recv.at[y, tp, c]), (True, stage.at[tp, c], t_recv.at[tp, c])
            ):
                kind = (s != y) if staged else (s == y)
                if dz:

                    @pl.when(kind)
                    def _():
                        remote(part, dst, y_send.at[dz, c], sem, (k, fs, p)).start()
                else:

                    @pl.when(kind & (p == tp))
                    def _():
                        pltpu.make_async_copy(part, dst, sem).start()

                    @pl.when(kind & (p != tp))
                    def _():
                        remote(part, dst, y_send.at[dz, c], sem, partner).start()

    passed = []

    def forward(c):
        for h in range(2):
            slot = stage.at[h, c]
            remote(slot, slot, y_send.at[0, 0], t_recv.at[h, c], partner).wait_recv()
            move = remote(slot, yg.at[y, h, c], t_send.at[h, c], y_recv.at[y, h, c], peer)
            move.start()
            passed.append(move)

    def multiply(c):
        gives = []
        for h in range(2):
            for q in range(2):
                slot = yg.at[q, h, c]
                remote(slot, slot, y_send.at[0, 0], y_recv.at[q, h, c], partner).wait_recv()
            k = 2 * h + c
            for f in range(nfs):
                acc = jnp.zeros((few2, block), jnp.float32)
                for q in range(2):
                    for b in range(2):
                        acc += jnp.dot(
                            yg[q, h, c, :, b * group : (b + 1) * group],
                            backs[f, b, q * group : (q + 1) * group, :],
                            preferred_element_type=jnp.float32,
                        )
                accs[k, :, f * block : (f + 1) * block] = acc
            give[k] = accs[k, pl.ds(pl.multiple_of((1 - tp) * few, few), few), :].astype(jnp.bfloat16)
            move = remote(give.at[k], take.at[k], g_send.at[k], g_recv.at[k], partner)
            move.start()
            gives.append(move)
        return gives

    def finish(c, gives):
        for h in range(2):
            k = 2 * h + c
            gives[h].wait()
            own = accs[k, pl.ds(pl.multiple_of(tp * few, few), few), :]
            done[k] = (own + take[k].astype(jnp.float32)).astype(jnp.bfloat16)
            dst = out.at[:, cols(sp, across)]

            @pl.when(sp == k)
            def _():
                pltpu.make_async_copy(done.at[k], dst, o_recv.at[sp]).start()

            @pl.when(sp != k)
            def _():
                remote(done.at[k], dst, o_send.at[k], o_recv.at[sp], (k, fs, tp)).start()

    forward(0)
    first = multiply(0)
    finish(0, first)
    forward(1)
    second = multiply(1)
    finish(1, second)

    for k in range(nsp):
        view = out.at[:, k * across : (k + 1) * across]
        remote(done.at[k], view, o_send.at[k], o_recv.at[k], partner).wait_recv()

        @pl.when(sp != k)
        def _():
            remote(done.at[k], view, o_send.at[k], o_recv.at[k], partner).wait_send()

    for c in range(2):
        slot = yg.at[0, 0, c]
        for dz in range(1, nsp):
            remote(slot, slot, y_send.at[dz, c], y_recv.at[0, 0, c], partner).wait_send()

        @pl.when(p != tp)
        def _():
            remote(slot, slot, y_send.at[0, c], y_recv.at[0, 0, c], partner).wait_send()

    for move in passed:
        move.wait_send()


def turned(values, cosine, sine):
    half_dim = values.shape[-1] // 2
    a, b = values[:, :half_dim], values[:, half_dim:]
    return jnp.concatenate([a * cosine - b * sine, a * sine + b * cosine], axis=-1)


def angles_of(positions, half_dim):
    inv_freq = 1.0 / rope_base ** jnp.linspace(0.0, 1.0, half_dim, dtype=jnp.float32)
    angles = positions.astype(jnp.float32)[:, None] * inv_freq[None, :]
    return jnp.cos(angles), jnp.sin(angles)


def paired(
    tokens, norm_gain, pool_proj, query_proj, key_proj, value_proj, pool_map, pool_scale,
    decay_rate, start_state, pool_back, retention_back,
):
    bf, f32 = jnp.bfloat16, jnp.float32
    sp, fs, tp, y, x = where_am_i()
    nsp = lax.axis_size("sp")
    tok = tokens[0]
    span, width = tok.shape
    rows, two = pool_proj.shape
    group = two // 2
    length = nsp * span
    half = length // 2
    vm, hbm = pl.BlockSpec(memory_space=pltpu.VMEM), pl.BlockSpec(memory_space=pl.ANY)
    dma = pltpu.SemaphoreType.DMA
    rs = start_state.shape[2]
    joined, start, backs = pl.pallas_call(
        project_kernel,
        out_shape=(
            jax.ShapeDtypeStruct((4, length, group), bf),
            jax.ShapeDtypeStruct((nsp * rs, group), bf),
            jax.ShapeDtypeStruct((4, 2) + pool_back.shape, bf),
        ),
        in_specs=[vm, vm, hbm, hbm, hbm, hbm, hbm, hbm, hbm],
        out_specs=(vm, vm, vm),
        scratch_shapes=[
            pltpu.VMEM((span, width), bf),
            pltpu.VMEM((2, nsp * span, width // nsp), bf),
            pltpu.VMEM((4, 4, rows, group), bf),
            pltpu.VMEM((4, 2, length, group), bf),
            pltpu.VMEM((4, nsp, half, group), bf),
            dma((3, 4)), dma((4, 4)), dma((4,)), dma((7,)), dma((2, nsp)), dma,
            dma((7,)), dma((7,)), dma((4,)), dma((nsp,)), dma((3, 2)), dma((4, 2)), dma((2,)),
            dma((4, 4)), dma((4, nsp)), dma((4,)), dma((4,)),
        ],
        compiler_params=pltpu.CompilerParams(collective_id=0, has_side_effects=True, vmem_limit_bytes=60 * 2**20),
        name="project",
    )(
        tok, norm_gain[None, :], pool_proj, query_proj, key_proj, value_proj,
        start_state[0].astype(bf), pool_back, retention_back,
    )
    mine = lax.dynamic_slice_in_dim(joined[1], tp * half, half, 0)
    head = 2 * (sp % 2) + y
    local = lax.dynamic_index_in_dim(decay_rate, y, 0, keepdims=False)
    other = lax.ppermute(decay_rate, "tp", [(0, 1), (1, 0)])
    rate = jnp.where(sp % 2 == tp, local, lax.dynamic_index_in_dim(other, y, 0, keepdims=False))
    every = jnp.arange(length, dtype=jnp.int32)
    position = tp * half + jnp.arange(half, dtype=jnp.int32)

    pool_all = jnp.concatenate([jnp.zeros((HALO, group), f32), joined[0].astype(f32)], axis=0)
    extended = lax.dynamic_slice_in_dim(pool_all, tp * half, half + HALO, 0)
    sums = trailing_sums(extended, half)
    windows = jnp.array(window_list, dtype=jnp.int32)
    chosen = sums[0]
    for i in range(1, GROUPS):
        chosen = jnp.where(head == i, sums[i], chosen)
    counts = jnp.minimum(windows[head], position + 1).astype(f32)
    differ = (chosen / counts[:, None] - extended[HALO:]).astype(bf)
    this_map = lax.dynamic_index_in_dim(pool_map, head, 0, keepdims=False)
    scale = lax.dynamic_slice_in_dim(pool_scale, head * group, group, 0)
    pool_out = (jnp.dot(differ, this_map, preferred_element_type=f32) * scale).astype(bf)

    cosine, sine = angles_of(every, group // 2)
    my_cos = lax.dynamic_slice_in_dim(cosine, tp * half, half, 0)
    my_sin = lax.dynamic_slice_in_dim(sine, tp * half, half, 0)
    rq = turned(mine.astype(f32), my_cos, my_sin)
    rk = turned(joined[2].astype(f32), cosine, sine) * group ** (-0.5)
    value = joined[3].astype(f32)
    gap = (position[:, None] - every[None, :]).astype(f32)
    mask = jnp.where(gap >= 0, jnp.exp(-jnp.maximum(gap, 0.0) * rate), 0.0)
    high = lax.Precision.HIGHEST
    scores = jnp.dot(rq, rk.T, precision=high) * mask
    fade = jnp.exp(-(position.astype(f32) + 1.0) * rate)
    ret = jnp.dot(scores, value, precision=high) + jnp.dot(
        rq * fade[:, None], start.astype(f32), precision=high
    )
    ret = ret * lax.rsqrt(jnp.mean(ret * ret, axis=-1, keepdims=True) + eps)
    yh = jnp.concatenate([pool_out, ret.astype(bf)], axis=1)

    few = span // 2
    return pl.pallas_call(
        output_kernel,
        out_shape=jax.ShapeDtypeStruct((few, width), bf),
        in_specs=[vm, vm],
        out_specs=vm,
        scratch_shapes=[
            pltpu.VMEM((2, 2, 2, span, 2 * group), bf),
            pltpu.VMEM((2, 2, span, 2 * group), bf),
            pltpu.VMEM((nsp, span, 4 * pool_back.shape[1]), f32),
            pltpu.VMEM((nsp, few, 4 * pool_back.shape[1]), bf),
            pltpu.VMEM((nsp, few, 4 * pool_back.shape[1]), bf),
            pltpu.VMEM((nsp, few, 4 * pool_back.shape[1]), bf),
            dma((nsp, 2)), dma((2, 2, 2)), dma((2, 2)), dma((2, 2)), dma((nsp,)), dma((nsp,)), dma((nsp,)), dma((nsp,)),
        ],
        compiler_params=pltpu.CompilerParams(collective_id=1, has_side_effects=True, vmem_limit_bytes=60 * 2**20),
        name="output",
    )(yh, backs)[None]


def solution(mesh):
    sizes = mesh.shape
    small = sizes["sp"] == 4 and sizes["fs"] == 4 and sizes["tp"] == 2
    placed = (
        P("fs", "sp", None),
        P(),
        P(("sp", "fs"), "tp"),
        P(("sp", "fs"), "tp"),
        P(("sp", "fs"), "tp"),
        P(("sp", "fs"), "tp"),
        P(),
        P(),
        P("tp"),
        P("fs", "tp", "sp", None),
        P("tp", ("sp", "fs")),
        P("tp", ("sp", "fs")),
    )
    return jax.shard_map(
        paired if small else on_device,
        mesh=mesh,
        in_specs=placed,
        out_specs=P("fs", ("sp", "tp"), None),
        check_vma=False,
    )
```

```python
import functools

from jax.experimental import pallas as pl
from jax.experimental.pallas import tpu as pltpu

import jax
import jax.numpy as jnp
from jax import lax
from jax.sharding import PartitionSpec as P

GROUPS = 4
BLOCK = 128
HALO = 16


eps = 1e-06
rope_base = 10000.0
highest_precision = lax.Precision.HIGHEST
window_list = (2, 4, 8, 16)


def shortened(x):
    return jax.tree.map(lambda a: a.astype(jnp.bfloat16) if a.dtype == jnp.float32 else a, x)


def shifted(x, axis, by):
    devices = lax.axis_size(axis)
    pairs = [(i, i + by) for i in range(devices) if 0 <= i + by < devices]
    return lax.ppermute(x, axis, pairs)


def carried_in(value, axis, join, neutral):
    count, mine = (lax.axis_size(axis), lax.axis_index(axis))
    pieces = jax.tree.map(lambda part: lax.all_gather(part, axis), value)
    running = jax.tree.map(
        lambda part, zero: jnp.full_like(part, 0) + jnp.asarray(zero, part.dtype), value, neutral
    )

    def turn(position, running):
        longer = join(running, jax.tree.map(lambda part: part[position], pieces))
        return jax.tree.map(lambda new, old: jnp.where(position < mine, new, old), longer, running)

    return lax.fori_loop(0, count - 1, turn, running)


def rotate(values, positions):
    half_dim = values.shape[-1] // 2
    inv_freq = 1.0 / rope_base ** jnp.linspace(0.0, 1.0, half_dim, dtype=jnp.float32)
    angles = positions.astype(jnp.float32)[:, None] * inv_freq[None, :]
    cosine = jnp.cos(angles)[:, None, :]
    sine = jnp.sin(angles)[:, None, :]
    first_half = values[..., :half_dim]
    second_half = values[..., half_dim:]
    return jnp.concatenate(
        [first_half * cosine - second_half * sine, first_half * sine + second_half * cosine],
        axis=-1,
    )


def trailing_sums(extended, length):
    begin = extended.shape[0] - length
    running = extended[begin:]
    results = []
    for behind in range(1, 16):
        running = running + extended[begin - behind : begin - behind + length]
        if behind + 1 in window_list:
            results.append(running)
    return results


def reshape_blocks(array):
    return array.reshape((array.shape[0] // BLOCK, BLOCK) + array.shape[1:])


def block_retention(queries, keys_in, values_in, decay_rate, initial):
    length, head_count, head_dim = queries.shape
    within = jnp.arange(BLOCK, dtype=jnp.float32)
    distance = within[:, None] - within[None, :]
    decay_mask = jnp.where(
        distance[None] >= 0,
        jnp.exp(-jnp.maximum(distance, 0.0)[None] * decay_rate[:, None, None]),
        0.0,
    )
    query_decay_factor = jnp.exp(-(within + 1.0)[:, None] * decay_rate[None, :])
    key_decay_factor = jnp.exp(-(BLOCK - 1.0 - within)[:, None] * decay_rate[None, :])
    block_decay_factor = jnp.exp(-BLOCK * decay_rate)

    def advance(state_carry, inputs):
        block_queries, block_keys, block_values = inputs
        scores = (
            jnp.einsum("ihk,jhk->hij", block_queries, block_keys, precision=highest_precision)
            * decay_mask
        )
        inside = jnp.einsum("hij,jhv->ihv", scores, block_values, precision=highest_precision)
        across_blocks = jnp.einsum(
            "bzy,zyx->bzx",
            block_queries * query_decay_factor[:, :, None],
            state_carry,
            precision=highest_precision,
        )
        state_carry = state_carry * block_decay_factor[:, None, None] + jnp.einsum(
            "flm,fld->lmd",
            block_keys * key_decay_factor[:, :, None],
            block_values,
            precision=highest_precision,
        )
        return (state_carry, inside + across_blocks)

    final_state, outputs = lax.scan(
        advance,
        initial,
        (reshape_blocks(queries), reshape_blocks(keys_in), reshape_blocks(values_in)),
    )
    return (outputs.reshape(length, head_count, values_in.shape[-1]), final_state)


def combine_states(earlier, latter):
    return (earlier[0] * latter[0], latter[0][:, None, None] * earlier[1] + latter[1])


def on_device(
    tokens,
    norm_gain,
    pool_proj,
    query_proj,
    key_proj,
    value_proj,
    pool_map,
    pool_scale,
    decay_rate,
    start_state,
    pool_back,
    retention_back,
):
    sequence = tokens[0]
    length = sequence.shape[0]
    tp_index = lax.axis_index("tp")
    sp_index = lax.axis_index("sp")
    tp_count = lax.axis_size("tp")
    floats = sequence.astype(jnp.float32)
    normed = (
        floats * lax.rsqrt(jnp.mean(floats * floats, axis=-1, keepdims=True) + eps) * norm_gain
    ).astype(jnp.bfloat16)
    group_normed = lax.all_gather(normed, "fs", axis=0, tiled=True)
    quarters = (
        lax.all_to_all(pool_proj, "fs", split_axis=1, concat_axis=0, tiled=True),
        lax.all_to_all(query_proj, "fs", split_axis=1, concat_axis=0, tiled=True),
        lax.all_to_all(key_proj, "fs", split_axis=1, concat_axis=0, tiled=True),
        lax.all_to_all(value_proj, "fs", split_axis=1, concat_axis=0, tiled=True),
    )
    pieces = (
        lax.all_gather(quarters[0], "sp", axis=0, tiled=True),
        lax.all_gather(quarters[1], "sp", axis=0, tiled=True),
        lax.all_gather(quarters[2], "sp", axis=0, tiled=True),
        lax.all_gather(quarters[3], "sp", axis=0, tiled=True),
    )
    partial_cols = tuple(
        (jnp.dot(group_normed, piece_w, preferred_element_type=jnp.float32) for piece_w in pieces)
    )
    rounded = tuple((result.astype(jnp.bfloat16) for result in partial_cols))
    pool_in, query_bf, key_bf, value_bf = jax.tree.map(
        lambda part, own: part.astype(own.dtype),
        lax.all_to_all(shortened(rounded), "fs", split_axis=0, concat_axis=1, tiled=True),
        rounded,
    )
    positions = jnp.arange(length, dtype=jnp.int32) + sp_index * length
    before = shifted(pool_in[length - HALO :], "sp", 1)
    extended = jnp.concatenate([before, pool_in], axis=0).astype(jnp.float32)
    stacked = jnp.stack(trailing_sums(extended, length))
    local_groups = GROUPS // tp_count
    channels = pool_in.shape[1]
    group_dim = channels // local_groups
    group_maps = lax.dynamic_slice_in_dim(pool_map, tp_index * local_groups, local_groups, 0)
    scales = lax.dynamic_slice_in_dim(pool_scale, tp_index * channels, channels, 0)
    windows = jnp.array(window_list, dtype=jnp.int32)
    pieces = []
    for group_idx in range(local_groups):
        chosen_group = tp_index * local_groups + group_idx
        lower = group_idx * group_dim
        chosen = lax.dynamic_index_in_dim(stacked, chosen_group, 0, keepdims=False)[
            :, lower : lower + group_dim
        ]
        counts = jnp.minimum(windows[chosen_group], positions + 1).astype(jnp.float32)
        inputs = extended[HALO:, lower : lower + group_dim]
        differ = (chosen / counts[:, None] - inputs).astype(jnp.bfloat16)
        pieces.append(jnp.dot(differ, group_maps[group_idx], preferred_element_type=jnp.float32))
    pool_out = (jnp.concatenate(pieces, axis=1) * scales).astype(jnp.bfloat16)
    head_count = decay_rate.shape[0]
    head_dim = query_bf.shape[1] // head_count
    queries = rotate(query_bf.astype(jnp.float32).reshape(length, head_count, head_dim), positions)
    keys_in = rotate(
        key_bf.astype(jnp.float32).reshape(length, head_count, head_dim), positions
    ) * head_dim ** (-0.5)
    values_in = value_bf.astype(jnp.float32).reshape(length, head_count, head_dim)
    zeros_state = jnp.zeros((head_count, head_dim, head_dim), jnp.float32)
    local_output, local_state = block_retention(
        queries, keys_in, values_in, decay_rate, zeros_state
    )
    span_decay = jnp.exp(-decay_rate * length)
    whole_start = lax.all_gather(start_state, "sp", axis=2, tiled=True)[0]
    span_factor, carried_over = carried_in(
        (span_decay, local_state), "sp", combine_states, (jnp.ones_like(span_decay), zeros_state)
    )
    offset_float = (sp_index * length).astype(jnp.float32)
    carried_over = carried_over + jnp.exp(-decay_rate * offset_float)[:, None, None] * whole_start
    steps_in = jnp.arange(length, dtype=jnp.float32) + 1.0
    query_rows_scaled = queries * jnp.exp(-steps_in[:, None] * decay_rate[None, :])[:, :, None]
    retained_output = local_output + jnp.einsum(
        "lpi,pib->lpb", query_rows_scaled, carried_over, precision=highest_precision
    )
    retained_output = retained_output * lax.rsqrt(
        jnp.mean(retained_output * retained_output, axis=-1, keepdims=True) + eps
    )
    ret_out = retained_output.reshape(length, head_count * head_dim).astype(jnp.bfloat16)
    pool_cols, retention_cols = (
        lax.all_gather(pool_back, ("sp", "fs"), axis=1, tiled=True),
        lax.all_gather(retention_back, ("sp", "fs"), axis=1, tiled=True),
    )
    weight_local = jnp.concatenate([pool_cols, retention_cols], axis=0)
    joined = jnp.concatenate([pool_out, ret_out], axis=1)
    mixed = lax.psum_scatter(
        jnp.dot(joined, weight_local, preferred_element_type=jnp.float32).astype(jnp.bfloat16),
        "tp",
        scatter_dimension=0,
        tiled=True,
    )
    return mixed[None]


MESH = pl.DeviceIdType.MESH


def where_am_i():
    sp, fs, tp = (lax.axis_index(name) for name in ("sp", "fs", "tp"))
    return sp, fs, tp, fs // 2, fs % 2


def remote(src, dst, send, recv, target):
    return pltpu.make_async_remote_copy(
        src_ref=src, dst_ref=dst, send_sem=send, recv_sem=recv, device_id=target, device_id_type=MESH
    )


def greet(others):
    barrier = pltpu.get_barrier_semaphore()
    for other in others:
        pl.semaphore_signal(barrier, inc=1, device_id=other, device_id_type=MESH)
    pl.semaphore_wait(barrier, len(others))


def cols(index, size):
    return pl.ds(pl.multiple_of(index * size, size), size)


def project_kernel(
    tok, gain, wp, wq, wk, wv, state, pb, rb,
    joined, start, backs,
    xn, xg, wg, part, got,
    w_send, w_recv, w_local, x_send, x_recv, x_local, f_send, f_recv,
    s_send, s_recv, b_send, b_recv, b_local, p_send, p_recv, j_send, j_recv,
):
    sp, fs, tp, y, x = where_am_i()
    nsp, nfs = 4, 4
    span, width = tok.shape
    half = span // 2
    feats = width // nsp
    rows, group = wg.shape[2], wg.shape[3]
    mats = (wp, wq, wk, wv)
    partner = (sp, fs, 1 - tp)
    waits = []
    greet(
        [
            (lax.rem(sp + dz, nsp), 2 * lax.rem(y + dy, 2) + x, lax.rem(tp + dt, 2))
            for dz in range(nsp) for dy in range(2) for dt in range(2) if dz or dy or dt
        ]
        + [(sp, 2 * lax.rem(y + dy, 2) + 1 - x, tp) for dy in range(2)]
    )

    def send_mat(m):
        for d in (3, 1, 2):
            to = lax.rem(fs + d, nfs)
            c = remote(
                mats[m].at[:, cols(to // 2, group)], wg.at[m, fs], w_send.at[d - 1, m],
                w_recv.at[m, fs], (sp, to, tp),
            )
            c.start()
            waits.append(c)
        c = pltpu.make_async_copy(mats[m].at[:, cols(y, group)], wg.at[m, fs], w_local.at[m])
        c.start()
        return c

    own_w = [send_mat(0)]

    floats = tok[...].astype(jnp.float32)
    xn[...] = (
        floats * lax.rsqrt(jnp.mean(floats * floats, axis=-1, keepdims=True) + eps) * gain[...]
    ).astype(jnp.bfloat16)

    mine = pl.ds(pl.multiple_of(tp * half, half), half)

    def slot_of(from_y, from_sp):
        return xg.at[from_y, pl.ds(pl.multiple_of(from_sp * span + tp * half, half), half)]

    peer = (sp, 2 * (1 - y) + x, tp)
    for dz in (2, 1, 3, 0):
        to_sp = lax.rem(sp + dz, nsp)
        c = remote(
            xn.at[mine, cols(to_sp, feats)], slot_of(y, sp), x_send.at[dz], x_recv.at[y, sp],
            (to_sp, fs, tp) if dz else peer,
        )
        c.start()
        waits.append(c)
    own_x = pltpu.make_async_copy(
        xn.at[:, cols(sp, feats)], xg.at[y, pl.ds(pl.multiple_of(sp * span, span), span)], x_local
    )
    own_x.start()
    forwards = []

    def arrived(from_y, from_sp, order):
        slot = slot_of(from_y, from_sp)
        remote(slot, slot, x_send.at[0], x_recv.at[from_y, from_sp], partner).wait_recv()
        c = remote(slot, slot, f_send.at[order], f_recv.at[order], partner)
        c.start()
        forwards.append(c)
        return slot

    for dz in (1, 3, 2):
        fr_sp = lax.rem(sp + nsp - dz, nsp)
        slot = arrived(y, fr_sp, dz - 1)
        c = remote(slot, slot, x_send.at[nsp + dz - 1], x_recv.at[y, fr_sp], peer)
        c.start()
        waits.append(c)
    for m in range(1, 4):
        own_w.append(send_mat(m))
    for j in range(2):
        for h in range(2):
            to_sp, to_fs = 2 * y + tp, 2 * j + x
            rs = state.shape[1]
            dst = start.at[pl.ds(pl.multiple_of(sp * rs, rs), rs)]
            same = (to_sp == sp) & (to_fs == fs) & (tp == h)

            @pl.when(same)
            def _():
                pltpu.make_async_copy(state.at[j], dst, s_recv.at[sp]).start()

            @pl.when(jnp.logical_not(same))
            def _():
                remote(state.at[j], dst, s_send.at[2 * j + h], s_recv.at[sp], (to_sp, to_fs, h)).start()

    own_b = []
    for b, back in enumerate((pb, rb)):
        c = pltpu.make_async_copy(back, backs.at[fs, b], b_local.at[b])
        c.start()
        own_b.append(c)
        for d in (3, 1, 2):
            to = lax.rem(fs + d, nfs)
            c = remote(back, backs.at[fs, b], b_send.at[d - 1, b], b_recv.at[fs, b], (sp, to, tp))
            c.start()
            waits.append(c)

    own_x.wait()
    for c in forwards:
        c.wait()
    early = len(forwards)

    tall = 2 * span
    for m in range(4):
        own_w[m].wait()
        for d in range(1, nfs):
            fr = lax.rem(fs + nfs - d, nfs)
            remote(
                mats[m].at[:, cols(y, group)], wg.at[m, fr], w_send.at[d - 1, m], w_recv.at[m, fr], partner
            ).wait_recv()
        for s in (y, 1 - y):
            if m == 0 and s is not y:
                for dz in (0, 1, 3, 2):
                    arrived(1 - y, lax.rem(sp + nsp - dz, nsp), 3 + dz)
                for c in forwards[early:]:
                    c.wait()
            acc = jnp.zeros((2 * tall, group), jnp.float32)
            for f in range(nfs):
                acc += jnp.dot(
                    xg[s, :, f * rows : (f + 1) * rows], wg[m, f], preferred_element_type=jnp.float32
                )
            part[m, s] = acc.astype(jnp.bfloat16)
            for h in range(2):
                same = (2 * s + tp == sp) & (tp == h)
                src = part.at[m, s, h * tall : (h + 1) * tall]

                @pl.when(same)
                def _():
                    pltpu.make_async_copy(src, got.at[m, sp], p_recv.at[m, sp]).start()

                @pl.when(jnp.logical_not(same))
                def _():
                    remote(
                        src, got.at[m, sp], p_send.at[m, 2 * s + h], p_recv.at[m, sp], (2 * s + tp, fs, h)
                    ).start()

    here = pl.ds(pl.multiple_of(tp * tall, tall), tall)
    there = pl.ds(pl.multiple_of((1 - tp) * tall, tall), tall)
    lasts = []
    for m in range(4):
        for k in range(nsp):
            remote(got.at[m, k], got.at[m, k], p_send.at[0, 0], p_recv.at[m, k], partner).wait_recv()
        total = got[m, 0].astype(jnp.float32)
        for k in range(1, nsp):
            total += got[m, k].astype(jnp.float32)
        joined[m, here] = total.astype(jnp.bfloat16)
        c = remote(joined.at[m, here], joined.at[m, here], j_send.at[m], j_recv.at[m], partner)
        c.start()
        lasts.append(c)
    for m in range(4):
        lasts[m].wait_send()
        remote(joined.at[m, there], joined.at[m, there], j_send.at[m], j_recv.at[m], partner).wait_recv()

    for j in range(2):
        for h in range(2):
            to_sp, to_fs = 2 * y + tp, 2 * j + x
            same = (to_sp == sp) & (to_fs == fs) & (tp == h)

            @pl.when(jnp.logical_not(same))
            def _():
                remote(state.at[j], start.at[pl.ds(0, state.shape[1])], s_send.at[2 * j + h], s_recv.at[0], partner).wait_send()

            same_p = (2 * j + tp == sp) & (tp == h)

            @pl.when(jnp.logical_not(same_p))
            def _():
                for m in range(4):
                    remote(got.at[m, 0], got.at[m, 0], p_send.at[m, 2 * j + h], p_recv.at[m, 0], partner).wait_send()

    for k in range(nsp):
        rs = state.shape[1]
        slot = start.at[k * rs : (k + 1) * rs]
        remote(slot, slot, s_send.at[0], s_recv.at[k], partner).wait_recv()
    for b, back in enumerate((pb, rb)):
        own_b[b].wait()
        for d in range(1, nfs):
            fr = lax.rem(fs + nfs - d, nfs)
            remote(back, backs.at[fr, b], b_send.at[d - 1, b], b_recv.at[fr, b], partner).wait_recv()
    for c in waits:
        c.wait_send()


def output_kernel(
    yh, backs, out,
    yg, stage, accs, give, take, done,
    y_send, y_recv, t_send, t_recv, g_send, g_recv, o_send, o_recv,
):
    sp, fs, tp, y, x = where_am_i()
    nsp, nfs = 4, 4
    half, wide = yh.shape
    group = wide // 2
    block = backs.shape[3]
    few = out.shape[0]
    across = nfs * block
    partner = (sp, fs, 1 - tp)
    s, p = sp // 2, sp % 2
    peer = (sp, 2 * (1 - y) + x, tp)
    greet(
        [
            (lax.rem(sp + dz, nsp), fs, lax.rem(tp + dt, 2))
            for dz in range(nsp) for dt in range(2) if dz or dt
        ]
        + [peer]
    )
    few2 = half // 2
    for c in range(2):
        part = yh.at[c * few2 : (c + 1) * few2]
        for dz in (2, 1, 3, 0):
            k = lax.rem(sp + dz, nsp)
            for staged, dst, sem in (
                (False, yg.at[y, tp, c], y_recv.at[y, tp, c]), (True, stage.at[tp, c], t_recv.at[tp, c])
            ):
                kind = (s != y) if staged else (s == y)
                if dz:

                    @pl.when(kind)
                    def _():
                        remote(part, dst, y_send.at[dz, c], sem, (k, fs, p)).start()
                else:

                    @pl.when(kind & (p == tp))
                    def _():
                        pltpu.make_async_copy(part, dst, sem).start()

                    @pl.when(kind & (p != tp))
                    def _():
                        remote(part, dst, y_send.at[dz, c], sem, partner).start()

    passed = []

    def forward(c):
        for h in range(2):
            slot = stage.at[h, c]
            remote(slot, slot, y_send.at[0, 0], t_recv.at[h, c], partner).wait_recv()
            move = remote(slot, yg.at[y, h, c], t_send.at[h, c], y_recv.at[y, h, c], peer)
            move.start()
            passed.append(move)

    def multiply(c):
        gives = []
        for h in range(2):
            for q in range(2):
                slot = yg.at[q, h, c]
                remote(slot, slot, y_send.at[0, 0], y_recv.at[q, h, c], partner).wait_recv()
            k = 2 * h + c
            for f in range(nfs):
                acc = jnp.zeros((few2, block), jnp.float32)
                for q in range(2):
                    for b in range(2):
                        acc += jnp.dot(
                            yg[q, h, c, :, b * group : (b + 1) * group],
                            backs[f, b, q * group : (q + 1) * group, :],
                            preferred_element_type=jnp.float32,
                        )
                accs[k, :, f * block : (f + 1) * block] = acc
            give[k] = accs[k, pl.ds(pl.multiple_of((1 - tp) * few, few), few), :].astype(jnp.bfloat16)
            move = remote(give.at[k], take.at[k], g_send.at[k], g_recv.at[k], partner)
            move.start()
            gives.append(move)
        return gives

    def finish(c, gives):
        for h in range(2):
            k = 2 * h + c
            gives[h].wait()
            own = accs[k, pl.ds(pl.multiple_of(tp * few, few), few), :]
            done[k] = (own + take[k].astype(jnp.float32)).astype(jnp.bfloat16)
            dst = out.at[:, cols(sp, across)]

            @pl.when(sp == k)
            def _():
                pltpu.make_async_copy(done.at[k], dst, o_recv.at[sp]).start()

            @pl.when(sp != k)
            def _():
                remote(done.at[k], dst, o_send.at[k], o_recv.at[sp], (k, fs, tp)).start()

    forward(0)
    first = multiply(0)
    finish(0, first)
    forward(1)
    second = multiply(1)
    finish(1, second)

    for k in range(nsp):
        view = out.at[:, k * across : (k + 1) * across]
        remote(done.at[k], view, o_send.at[k], o_recv.at[k], partner).wait_recv()

        @pl.when(sp != k)
        def _():
            remote(done.at[k], view, o_send.at[k], o_recv.at[k], partner).wait_send()

    for c in range(2):
        slot = yg.at[0, 0, c]
        for dz in range(1, nsp):
            remote(slot, slot, y_send.at[dz, c], y_recv.at[0, 0, c], partner).wait_send()

        @pl.when(p != tp)
        def _():
            remote(slot, slot, y_send.at[0, c], y_recv.at[0, 0, c], partner).wait_send()

    for move in passed:
        move.wait_send()


def turned(values, cosine, sine):
    half_dim = values.shape[-1] // 2
    a, b = values[:, :half_dim], values[:, half_dim:]
    return jnp.concatenate([a * cosine - b * sine, a * sine + b * cosine], axis=-1)


def angles_of(positions, half_dim):
    inv_freq = 1.0 / rope_base ** jnp.linspace(0.0, 1.0, half_dim, dtype=jnp.float32)
    angles = positions.astype(jnp.float32)[:, None] * inv_freq[None, :]
    return jnp.cos(angles), jnp.sin(angles)


def paired(
    tokens, norm_gain, pool_proj, query_proj, key_proj, value_proj, pool_map, pool_scale,
    decay_rate, start_state, pool_back, retention_back,
):
    bf, f32 = jnp.bfloat16, jnp.float32
    sp, fs, tp, y, x = where_am_i()
    nsp = lax.axis_size("sp")
    tok = tokens[0]
    span, width = tok.shape
    rows, two = pool_proj.shape
    group = two // 2
    length = nsp * span
    half = length // 2
    vm, hbm = pl.BlockSpec(memory_space=pltpu.VMEM), pl.BlockSpec(memory_space=pl.ANY)
    dma = pltpu.SemaphoreType.DMA
    rs = start_state.shape[2]
    joined, start, backs = pl.pallas_call(
        project_kernel,
        out_shape=(
            jax.ShapeDtypeStruct((4, length, group), bf),
            jax.ShapeDtypeStruct((nsp * rs, group), bf),
            jax.ShapeDtypeStruct((4, 2) + pool_back.shape, bf),
        ),
        in_specs=[vm, vm, hbm, hbm, hbm, hbm, hbm, hbm, hbm],
        out_specs=(vm, vm, vm),
        scratch_shapes=[
            pltpu.VMEM((span, width), bf),
            pltpu.VMEM((2, nsp * span, width // nsp), bf),
            pltpu.VMEM((4, 4, rows, group), bf),
            pltpu.VMEM((4, 2, length, group), bf),
            pltpu.VMEM((4, nsp, half, group), bf),
            dma((3, 4)), dma((4, 4)), dma((4,)), dma((7,)), dma((2, nsp)), dma,
            dma((7,)), dma((7,)), dma((4,)), dma((nsp,)), dma((3, 2)), dma((4, 2)), dma((2,)),
            dma((4, 4)), dma((4, nsp)), dma((4,)), dma((4,)),
        ],
        compiler_params=pltpu.CompilerParams(collective_id=0, has_side_effects=True, vmem_limit_bytes=60 * 2**20),
        name="project",
    )(
        tok, norm_gain[None, :], pool_proj, query_proj, key_proj, value_proj,
        start_state[0].astype(bf), pool_back, retention_back,
    )
    mine = lax.dynamic_slice_in_dim(joined[1], tp * half, half, 0)
    head = 2 * (sp % 2) + y
    local = lax.dynamic_index_in_dim(decay_rate, y, 0, keepdims=False)
    other = lax.ppermute(decay_rate, "tp", [(0, 1), (1, 0)])
    rate = jnp.where(sp % 2 == tp, local, lax.dynamic_index_in_dim(other, y, 0, keepdims=False))
    every = jnp.arange(length, dtype=jnp.int32)
    position = tp * half + jnp.arange(half, dtype=jnp.int32)

    pool_all = jnp.concatenate([jnp.zeros((HALO, group), f32), joined[0].astype(f32)], axis=0)
    extended = lax.dynamic_slice_in_dim(pool_all, tp * half, half + HALO, 0)
    sums = trailing_sums(extended, half)
    windows = jnp.array(window_list, dtype=jnp.int32)
    chosen = sums[0]
    for i in range(1, GROUPS):
        chosen = jnp.where(head == i, sums[i], chosen)
    counts = jnp.minimum(windows[head], position + 1).astype(f32)
    differ = (chosen / counts[:, None] - extended[HALO:]).astype(bf)
    this_map = lax.dynamic_index_in_dim(pool_map, head, 0, keepdims=False)
    scale = lax.dynamic_slice_in_dim(pool_scale, head * group, group, 0)
    pool_out = (jnp.dot(differ, this_map, preferred_element_type=f32) * scale).astype(bf)

    cosine, sine = angles_of(every, group // 2)
    my_cos = lax.dynamic_slice_in_dim(cosine, tp * half, half, 0)
    my_sin = lax.dynamic_slice_in_dim(sine, tp * half, half, 0)
    rq = turned(mine.astype(f32), my_cos, my_sin)
    rk = turned(joined[2].astype(f32), cosine, sine) * group ** (-0.5)
    value = joined[3].astype(f32)
    gap = (position[:, None] - every[None, :]).astype(f32)
    mask = jnp.where(gap >= 0, jnp.exp(-jnp.maximum(gap, 0.0) * rate), 0.0)
    high = lax.Precision.HIGHEST
    scores = jnp.dot(rq, rk.T, precision=high) * mask
    fade = jnp.exp(-(position.astype(f32) + 1.0) * rate)
    ret = jnp.dot(scores, value, precision=high) + jnp.dot(
        rq * fade[:, None], start.astype(f32), precision=high
    )
    ret = ret * lax.rsqrt(jnp.mean(ret * ret, axis=-1, keepdims=True) + eps)
    yh = jnp.concatenate([pool_out, ret.astype(bf)], axis=1)

    few = span // 2
    return pl.pallas_call(
        output_kernel,
        out_shape=jax.ShapeDtypeStruct((few, width), bf),
        in_specs=[vm, vm],
        out_specs=vm,
        scratch_shapes=[
            pltpu.VMEM((2, 2, 2, span, 2 * group), bf),
            pltpu.VMEM((2, 2, span, 2 * group), bf),
            pltpu.VMEM((nsp, span, 4 * pool_back.shape[1]), f32),
            pltpu.VMEM((nsp, few, 4 * pool_back.shape[1]), bf),
            pltpu.VMEM((nsp, few, 4 * pool_back.shape[1]), bf),
            pltpu.VMEM((nsp, few, 4 * pool_back.shape[1]), bf),
            dma((nsp, 2)), dma((2, 2, 2)), dma((2, 2)), dma((2, 2)), dma((nsp,)), dma((nsp,)), dma((nsp,)), dma((nsp,)),
        ],
        compiler_params=pltpu.CompilerParams(collective_id=1, has_side_effects=True, vmem_limit_bytes=60 * 2**20),
        name="output",
    )(yh, backs)[None]


def solution(mesh):
    sizes = mesh.shape
    small = sizes["sp"] == 4 and sizes["fs"] == 4 and sizes["tp"] == 2
    placed = (
        P("fs", "sp", None),
        P(),
        P(("sp", "fs"), "tp"),
        P(("sp", "fs"), "tp"),
        P(("sp", "fs"), "tp"),
        P(("sp", "fs"), "tp"),
        P(),
        P(),
        P("tp"),
        P("fs", "tp", "sp", None),
        P("tp", ("sp", "fs")),
        P("tp", ("sp", "fs")),
    )
    return jax.shard_map(
        paired if small else on_device,
        mesh=mesh,
        in_specs=placed,
        out_specs=P("fs", ("sp", "tp"), None),
        check_vma=False,
    )
```
